32 devices in a mesh: ep: 4 (over y, x), tp: 8 (over z, core).
Axes of the slice: x: 2, y: 2, z: 4, core: 2. Of those that a mesh axis runs over, the one named last changes fastest.
Arguments:
- residual: bfloat16 [128, 2048], P('ep'), may hold values from -6 to 6
- mixer_gain: float32 [2048], replicated, may hold values from 0.1 to 1.9
- gate_proj: bfloat16 [2048, 2048], P('ep', 'tp'), may hold values from -0.125 to 0.125
- input_proj: bfloat16 [2048, 2048], P('ep', 'tp'), may hold values from -0.125 to 0.125
- write_proj: bfloat16 [2048, 2048], P('ep', 'tp'), may hold values from -0.125 to 0.125
- read_proj: bfloat16 [2048, 2048], P('ep', 'tp'), may hold values from -0.125 to 0.125
- step_proj: bfloat16 [2048, 32], replicated, may hold values from -0.125 to 0.125
- conv_weight: float32 [4, 3, 2048], replicated, may hold values from -3 to 3
- step_bias: float32 [32], replicated, may hold values from -4 to 0
- log_rate: float32 [32], replicated, may hold values from 0 to 2.5
- skip_gain: float32 [32], replicated, may hold values from -4 to 4
- group_gain: float32 [2048], replicated, may hold values from 0.1 to 1.9
- ssm_state: float32 [128, 32, 64, 128], P('ep', 'tp'), may hold values from -2 to 2
- conv_state: bfloat16 [128, 3, 3, 2048], P('ep', None, None, 'tp'), may hold values from -6 to 6
- out_proj: bfloat16 [2048, 2048], P('tp'), may hold values from -0.125 to 0.125
- ffn_gain: float32 [2048], replicated, may hold values from 0.1 to 1.9
- routes: int32 [128, 2], P('ep'), may hold values from 0 to 7, all different within a row; in each aligned block of 32 rows (0 to 31, 32 to 63, ...) at most 16 rows name the same one
- route_weight: float32 [128, 2], P('ep'), may hold values from 0.2 to 1
- expert_gate: bfloat16 [8, 2048, 2048], P('ep', None, 'tp'), may hold values from -0.125 to 0.125
- expert_up: bfloat16 [8, 2048, 2048], P('ep', None, 'tp'), may hold values from -0.125 to 0.125
- expert_down: bfloat16 [8, 2048, 2048], P('ep', 'tp'), may hold values from -0.125 to 0.125
- dense_gate: bfloat16 [2048, 2048], P(None, 'tp'), may hold values from -0.125 to 0.125
- dense_up: bfloat16 [2048, 2048], P(None, 'tp'), may hold values from -0.125 to 0.125
- dense_down: bfloat16 [2048, 2048], P('tp'), may hold values from -0.125 to 0.125
- blend_weight: bfloat16 [2048], replicated, may hold values from -0.125 to 0.125
Outputs:
- layer_out: bfloat16 [128, 2048], P('ep', 'tp')
- new_state: float32 [128, 32, 64, 128], P('ep', 'tp')
- new_conv: bfloat16 [128, 3, 3, 2048], P('ep', None, None, 'tp')
The draws below stay inside these ranges and needn't reach their ends.
Inputs may be any that keep to these rules, and one draw needn't show every extreme that they name: `routes`: each row names 2 different experts. Within the 32 rows of one index of ep no expert is named by more than 16 rows, and in some such block some expert is named by exactly 16 rows.
All inputs are finite; a program needn't handle non-finite values.
Results may differ from the reference program's by a relative error of at most 0.015.
Values may be sent and summed in bfloat16 or wider, within the bound.
No kernel may reach another device: no remote copies, remote signals or barrier semaphores. Data moves between devices by JAX's collectives and lax.ppermute only.
A program may use at most 128 MiB of HBM per device.

```python
import math
import jax
import jax.numpy as jnp
import numpy as np
from jax import lax

D = 2048
HEADS = 32
HEAD_DIM = 64
GROUPS = 16
STATE = 128
KERNEL = 4
TOPK = 2
FFE = 2048
FFD = 2048
S_DEV = 32
D_INNER = 2048
EXPERTS = 8
TOK = 128
CAP = 16
N_EP = 4


def block_levels(stream_key, extent, pieces, smallest, high):
    loudness, own = 1.0, jax.random.fold_in(stream_key, 6)
    for position, shards_of in pieces:
        draws = jnp.exp(jax.random.uniform(jax.random.fold_in(own, position), (shards_of,), jnp.float32, smallest / len(pieces), high / len(pieces)))
        loudness = loudness * jnp.repeat(draws, extent[position] // shards_of).reshape([-1 if axis == position else 1 for axis in range(len(extent))])
    return loudness


def shared_out(key, own, number, rows, number_of, top, reach, lean):
    order = jax.random.permutation(key, number_of)
    heavy_load, ordinary = portions_of(number_of, rows * top, reach, lean, True), portions_of(number_of, rows * top, reach, lean, False)
    places = jnp.arange(number_of)

    def named(sizes, offset_by):
        used = int((sizes > 0).sum())
        fixed = max(1, used // 4)
        moved = fixed + (places - fixed + offset_by * (used - fixed)) % max(1, number_of - fixed)
        return jnp.zeros((number_of,), jnp.int32).at[order[jnp.where(places < fixed, places, moved)]].set(jnp.asarray(sizes, jnp.int32))

    sizes = jnp.where(number % 4 == 0, named(heavy_load, number // 4), named(ordinary, number - number // 4 - 1))
    mixed = jax.random.permutation(jax.random.fold_in(own, 3), number_of)
    giver, sink = mixed[0:number_of // 2 * 2:2], mixed[1:number_of // 2 * 2:2]
    margin = jnp.minimum(sizes[giver] - 1, reach - sizes[sink]) // 2
    margin = jnp.where((giver == order[0]) | (sink == order[0]) | (sizes[sink] == 0), 0, jnp.maximum(margin, 0))
    moved = jax.random.randint(jax.random.fold_in(own, 4), (number_of // 2,), 0, 1 << 20) % (margin + 1)
    sizes = sizes.at[giver].add(-moved).at[sink].add(moved)
    labels = jnp.searchsorted(jnp.cumsum(sizes), jnp.arange(rows * top), side="right").astype(jnp.int32)
    table = labels.reshape(top, rows).T
    table = table[jax.random.permutation(jax.random.fold_in(own, 1), rows)]
    offset_by = jax.random.randint(jax.random.fold_in(own, 2), (rows, 1), 0, top)
    return jnp.take_along_axis(table, (jnp.arange(top)[None, :] + offset_by) % top, axis=1)


def portions_of(amount, total, reach, skew, full):
    loads = [(1 << 20) // math.isqrt(rank ** skew) + 1 for rank in range(1, amount + 1)]
    largest = reach if full else min(reach, max(-(-total // amount), total * loads[0] // sum(loads)))
    least = 1 if total - largest >= amount - 1 else 0
    holding, surplus = [largest] + [least] * (amount - 1), total - largest - least * (amount - 1)
    while surplus > 0:
        candidates = [i for i in range(1, amount) if holding[i] < largest] or [i for i in range(1, amount) if holding[i] < reach]
        whole, left = sum([loads[i] for i in candidates]), surplus
        for i in candidates:
            more = min(reach - holding[i], max(1, left * loads[i] // whole), surplus)
            holding[i] = holding[i] + more
            surplus = surplus - more
    return np.array(holding)


def gaussian(key, dims, deviation, limit, cuts=(), held_as=jnp.bfloat16):
    values = deviation * jax.random.normal(key, dims, jnp.float32)
    if cuts:
        values = values * block_levels(key, dims, cuts, -0.22, 0.18)
    return jnp.clip(values, -limit, limit).astype(held_as)


def setup_inputs(seed: int = 0) -> dict:
    key_list = jax.random.split(jax.random.key(seed), 26)
    residual = gaussian(key_list[0], (TOK, D), 1.0, 6.0, ((0, 4),))
    mixer_gain = jnp.clip(1.0 + 0.18 * jax.random.normal(key_list[1], (D,), jnp.float32), 0.1, 1.9)
    gate_proj = gaussian(key_list[2], (D, D_INNER), D ** -0.5, 0.125, ((0, 4), (1, 8)))
    input_proj = gaussian(key_list[3], (D, D_INNER), D ** -0.5, 0.125, ((0, 4), (1, 8)))
    write_proj = gaussian(key_list[4], (D, D_INNER), D ** -0.5, 0.125, ((0, 4), (1, 8)))
    read_proj = gaussian(key_list[5], (D, D_INNER), D ** -0.5, 0.125, ((0, 4), (1, 8)))
    step_proj = gaussian(key_list[6], (D, HEADS), D ** -0.5, 0.125)
    conv_weight = gaussian(key_list[7], (KERNEL, 3, D_INNER), 0.5, 3.0, (), jnp.float32)
    step_bias = jnp.clip(jax.random.uniform(key_list[8], (HEADS,), jnp.float32, -4.0, 0.0), -4.0, 0.0)
    log_rate = jnp.clip(jax.random.uniform(key_list[9], (HEADS,), jnp.float32, 0.0, 2.5), 0.0, 2.5)
    skip_gain = gaussian(key_list[10], (HEADS,), 1.0, 4.0, (), jnp.float32)
    group_gain = jnp.clip(1.0 + 0.18 * jax.random.normal(key_list[11], (D_INNER,), jnp.float32), 0.1, 1.9)
    ssm_state = gaussian(key_list[12], (TOK, HEADS, HEAD_DIM, STATE), 0.3, 2.0, ((0, 4), (1, 8)), jnp.float32)
    conv_state = gaussian(key_list[13], (TOK, KERNEL - 1, 3, D_INNER), 1.0, 6.0, ((0, 4), (3, 8)))
    out_proj = gaussian(key_list[14], (D_INNER, D), D_INNER ** -0.5, 0.125, ((0, 8),))
    ffn_gain = jnp.clip(1.0 + 0.18 * jax.random.normal(key_list[15], (D,), jnp.float32), 0.1, 1.9)
    routes_keys = jax.random.split(jax.random.fold_in(key_list[16], 1), TOK // S_DEV)
    routes_turns = jax.random.permutation(jax.random.fold_in(key_list[16], 3), TOK // S_DEV)
    routes = jax.vmap(lambda own, number: shared_out(jax.random.fold_in(key_list[16], 2), own, number, S_DEV, EXPERTS, TOPK, CAP, 2))(routes_keys, routes_turns).reshape((TOK, TOPK))
    route_weight = jnp.clip(0.2 + 0.8 * jax.random.uniform(key_list[17], (TOK, TOPK), jnp.float32) ** block_levels(key_list[17], (TOK, TOPK), ((0, 4),), -0.2, 0.2), 0.2, 1.0)
    expert_gate = gaussian(key_list[18], (EXPERTS, D, FFE), D ** -0.5, 0.125, ((0, 4), (2, 8)))
    expert_up = gaussian(key_list[19], (EXPERTS, D, FFE), D ** -0.5, 0.125, ((0, 4), (2, 8)))
    expert_down = gaussian(key_list[20], (EXPERTS, FFE, D), FFE ** -0.5, 0.125, ((0, 4), (1, 8)))
    dense_gate = gaussian(key_list[21], (D, FFD), D ** -0.5, 0.125, ((1, 8),))
    dense_up = gaussian(key_list[22], (D, FFD), D ** -0.5, 0.125, ((1, 8),))
    dense_down = gaussian(key_list[23], (FFD, D), FFD ** -0.5, 0.125, ((0, 8),))
    blend_weight = gaussian(key_list[24], (D,), D ** -0.5, 0.125)
    return {"residual": residual, "mixer_gain": mixer_gain, "gate_proj": gate_proj, "input_proj": input_proj, "write_proj": write_proj, "read_proj": read_proj, "step_proj": step_proj, "conv_weight": conv_weight, "step_bias": step_bias, "log_rate": log_rate, "skip_gain": skip_gain, "group_gain": group_gain, "ssm_state": ssm_state, "conv_state": conv_state, "out_proj": out_proj, "ffn_gain": ffn_gain, "routes": routes, "route_weight": route_weight, "expert_gate": expert_gate, "expert_up": expert_up, "expert_down": expert_down, "dense_gate": dense_gate, "dense_up": dense_up, "dense_down": dense_down, "blend_weight": blend_weight}


epsilon = 1e-06

def rms_rows(values, gain_vector):
    floats_in = values.astype(jnp.float32)
    return floats_in * lax.rsqrt(lax.optimization_barrier(jnp.mean(floats_in * floats_in, axis=-1, keepdims=True)) + epsilon) * gain_vector

def reference(residual, mixer_gain, gate_proj, input_proj, write_proj, read_proj, step_proj, conv_weight, step_bias, log_rate, skip_gain, group_gain, ssm_state, conv_state, out_proj, ffn_gain, routes, route_weight, expert_gate, expert_up, expert_down, dense_gate, dense_up, dense_down, blend_weight):
    normed = rms_rows(residual, mixer_gain).astype(jnp.bfloat16)
    z_proj = jnp.dot(normed, gate_proj, preferred_element_type=jnp.float32).astype(jnp.bfloat16)
    x_proj = jnp.dot(normed, input_proj, preferred_element_type=jnp.float32).astype(jnp.bfloat16)
    b_proj = jnp.dot(normed, write_proj, preferred_element_type=jnp.float32).astype(jnp.bfloat16)
    c_proj = jnp.dot(normed, read_proj, preferred_element_type=jnp.float32).astype(jnp.bfloat16)
    step_raw = jnp.dot(normed, step_proj, preferred_element_type=jnp.float32)
    newest = jnp.stack((x_proj, b_proj, c_proj), axis=1)[:, None]
    stacked = jnp.concatenate((conv_state, newest), axis=1)
    new_conv = stacked[:, 1:]
    activated = jax.nn.silu(jnp.einsum('skcw,kcw->scw', stacked.astype(jnp.float32), conv_weight.astype(jnp.float32)))
    per_group = HEADS // GROUPS
    x_act = activated[:, 0].reshape(TOK, HEADS, HEAD_DIM)
    b_act = jnp.repeat(activated[:, 1].reshape(TOK, GROUPS, STATE), per_group, axis=1)
    c_act = jnp.repeat(activated[:, 2].reshape(TOK, GROUPS, STATE), per_group, axis=1)
    step_size = jax.nn.softplus(step_raw + step_bias)
    decay_factor = jnp.exp(-jnp.exp(log_rate) * step_size)
    new_state = decay_factor[:, :, None, None] * ssm_state + (step_size[:, :, None] * x_act)[..., None] * b_act[:, :, None, :]
    ssm_out = jnp.einsum('shpn,shn->shp', new_state, c_act) + skip_gain[None, :, None] * x_act
    gated_out = ssm_out.reshape(TOK, D_INNER) * jax.nn.silu(z_proj.astype(jnp.float32))
    grouped = gated_out.reshape(TOK, GROUPS, D_INNER // GROUPS)
    grouped = grouped * lax.rsqrt(lax.optimization_barrier(jnp.mean(grouped * grouped, axis=-1, keepdims=True)) + epsilon)
    mixed_out = (grouped.reshape(TOK, D_INNER) * group_gain).astype(jnp.bfloat16)
    resid_mid = (residual.astype(jnp.float32) + jnp.dot(mixed_out, out_proj, preferred_element_type=jnp.float32)).astype(jnp.bfloat16)
    normed_ffn = rms_rows(resid_mid, ffn_gain).astype(jnp.bfloat16)
    flat_routes = routes.reshape(N_EP, S_DEV * TOPK)
    onehot = (flat_routes[..., None] == jnp.arange(EXPERTS, dtype=jnp.int32)).astype(jnp.int32)
    slot_rank = lax.optimization_barrier(jnp.sum((jnp.cumsum(onehot, axis=1) - onehot) * onehot, axis=2)).astype(jnp.int32)
    source = jnp.broadcast_to(jnp.arange(N_EP, dtype=jnp.int32)[:, None], flat_routes.shape)
    repeated = jnp.repeat(normed_ffn, TOPK, axis=0).reshape(N_EP, S_DEV * TOPK, D)
    buffer = jnp.zeros((EXPERTS, N_EP, CAP, D), jnp.bfloat16).at[flat_routes, source, slot_rank].set(repeated)

    def expert(expert_args):
        expert_rows, w_gate, w_up, w_down = expert_args
        expert_rows = expert_rows.reshape(N_EP * CAP, D).astype(jnp.float32)
        gate_val = jnp.dot(expert_rows, w_gate.astype(jnp.float32))
        up_val = jnp.dot(expert_rows, w_up.astype(jnp.float32))
        hidden = (jax.nn.silu(gate_val) * up_val).astype(jnp.bfloat16)
        result = jnp.dot(hidden.astype(jnp.float32), w_down.astype(jnp.float32)).astype(jnp.bfloat16)
        return result.reshape(N_EP, CAP, D)
    results = lax.map(expert, (buffer, expert_gate, expert_up, expert_down))
    picked = results[flat_routes, source, slot_rank].astype(jnp.float32).reshape(TOK, TOPK, D)
    expert_mix = lax.optimization_barrier(jnp.sum(picked * route_weight[..., None], axis=1))
    gate_val = jnp.dot(normed_ffn, dense_gate, preferred_element_type=jnp.float32)
    up_val = jnp.dot(normed_ffn, dense_up, preferred_element_type=jnp.float32)
    dense_hidden = (jax.nn.silu(gate_val) * up_val).astype(jnp.bfloat16)
    dense_out = jnp.dot(dense_hidden, dense_down, preferred_element_type=jnp.float32)
    mix_weight = jax.nn.sigmoid(jnp.dot(normed_ffn, blend_weight, preferred_element_type=jnp.float32))
    layer_out = (resid_mid.astype(jnp.float32) + expert_mix + mix_weight[:, None] * dense_out).astype(jnp.bfloat16)
    return (layer_out, new_state, new_conv)
```

```python
import jax
import jax.numpy as jnp
from jax import lax
from jax.experimental import pallas as pl
from jax.experimental.pallas import tpu as pltpu
from jax.sharding import PartitionSpec as P

epsilon = 1e-06
CORES = 2
LANES = 128
F32 = jnp.float32
BF16 = jnp.bfloat16
EXACT = lax.Precision.HIGHEST


def partner(count, index, step):
    return index ^ step if count & (count - 1) == 0 else (index + step) % count


def send_ep(block, count, step, back=False):
    pairs = [(i, partner(count, i, step)) for i in range(count)]
    return lax.ppermute(block, "ep", [(b, a) for a, b in pairs] if back else pairs)


def send_z(block, count, step):
    pairs = [
        (z * CORES + c, partner(count, z, step) * CORES + c)
        for z in range(count)
        for c in range(CORES)
    ]
    return lax.ppermute(block, "tp", pairs)


def send_core(block, count):
    return lax.ppermute(block, "tp", [(i, i ^ 1) for i in range(count)])


def local_kernel(body, name, outs, operands, flops=0, scratch=()):
    whole = pl.BlockSpec(memory_space=pltpu.VMEM)
    return pl.pallas_call(
        body,
        name=name,
        out_shape=outs,
        in_specs=[whole] * len(operands),
        out_specs=jax.tree.map(lambda _: whole, outs),
        scratch_shapes=scratch,
        cost_estimate=pl.CostEstimate(flops=flops, bytes_accessed=0, transcendentals=0),
        compiler_params=pltpu.CompilerParams(vmem_limit_bytes=40 << 20),
    )(*operands)


def row_scale(values):
    return lax.rsqrt(jnp.mean(values * values, axis=-1, keepdims=True) + epsilon)


def halves(array, core, width):
    count = array.shape[1] // width
    even = jnp.concatenate([array[:, i * width : (i + 1) * width] for i in range(0, count, 2)], 1)
    odd = jnp.concatenate([array[:, i * width : (i + 1) * width] for i in range(1, count, 2)], 1)
    first = core == 0
    return jnp.where(first, even, odd), jnp.where(first, odd, even)


def interleave(mine, other, core, width):
    first = core == 0
    even, odd = jnp.where(first, mine, other), jnp.where(first, other, mine)
    parts = []
    for i in range(mine.shape[1] // width):
        parts += [even[:, i * width : (i + 1) * width], odd[:, i * width : (i + 1) * width]]
    return jnp.concatenate(parts, 1)


def pack_tokens(ep_count, expert_total, residual, mixer_gain, routes, route_weight):
    rows, model = residual.shape
    depth = model // ep_count
    side = -(-2 * expert_total // LANES) * LANES

    def body(res_ref, gain_ref, routes_ref, weight_ref, *outs):
        rank = lax.axis_index("ep")
        lane = lax.broadcasted_iota(jnp.int32, (rows, side), 1)
        named = jnp.where(lane < expert_total, lane, lane - expert_total)
        dense = jnp.zeros((rows, side), F32)
        for k in range(routes.shape[1]):
            dense = dense + jnp.where(
                routes_ref[:, k : k + 1] == named, weight_ref[:, k : k + 1], 0.0
            )
        high = dense.astype(BF16).astype(F32)
        dense = jnp.where(lane < expert_total, high, dense - high).astype(BF16)
        for step, out in enumerate(outs):
            start = pl.multiple_of(partner(ep_count, rank, step) * depth, LANES)
            cols = res_ref[:, pl.ds(start, depth)].astype(F32) * gain_ref[:, pl.ds(start, depth)]
            out[:, :depth] = cols.astype(BF16)
            out[:, depth:] = dense

    outs = [jax.ShapeDtypeStruct((rows, depth + side), BF16)] * ep_count
    return local_kernel(body, "pack_tokens", outs, (residual, mixer_gain, routes, route_weight))


def project(blocks, weights):
    rows = blocks[0].shape[0]
    depth, width = weights[0].shape
    count, kinds = len(blocks), len(weights)

    def body(*refs):
        ins, mats, outs = refs[:count], refs[count : count + kinds], refs[count + kinds :]
        stacked = jnp.concatenate([r[:, :depth] for r in ins], 0)
        for j, mat in enumerate(mats):
            result = jnp.dot(stacked, mat[...], preferred_element_type=F32)
            for i, out in enumerate(outs):
                piece = result[i * rows : (i + 1) * rows]
                out[:, j * width : (j + 1) * width] = piece.astype(out.dtype)

    outs = [jax.ShapeDtypeStruct((rows, kinds * width), BF16 if i else F32) for i in range(count)]
    flops = 2 * rows * count * depth * kinds * width
    return local_kernel(body, "project", outs, (*blocks, *weights), flops)


def head_terms(residual, mixer_gain, step_proj, step_bias, log_rate, skip_gain, heads, width):
    rows, model = residual.shape
    total = step_proj.shape[1]
    state = LANES

    def body(res_ref, gain_ref, proj_ref, bias_ref, rate_ref, skip_ref, scale, step, decay, skip, half):
        rank = lax.axis_index("tp")
        head_start = rank * heads
        values = res_ref[...].astype(F32)
        scaling = row_scale(values)
        normed = (values * scaling * gain_ref[...]).astype(BF16)
        raw = jnp.dot(normed, proj_ref[...], preferred_element_type=F32) + bias_ref[...]
        size = jnp.maximum(raw, 0.0) + jnp.log1p(jnp.exp(-jnp.abs(raw)))
        fade = jnp.exp(-jnp.exp(rate_ref[...]) * size)

        def spread(table, lanes):
            head = lax.broadcasted_iota(jnp.int32, (total, heads * lanes), 0) - head_start
            lane = lax.broadcasted_iota(jnp.int32, (total, heads * lanes), 1)
            hot = ((lane >= head * lanes) & (lane < (head + 1) * lanes)).astype(F32)
            return jnp.dot(table, hot, preferred_element_type=F32, precision=EXACT)

        scale[...] = jnp.broadcast_to(scaling, (rows, LANES))
        step[...] = spread(size, width // heads)
        decay[...] = spread(fade, state)
        skip[...] = spread(jnp.broadcast_to(skip_ref[...], (8, total)), width // heads)
        half[...] = halves(values, rank % CORES, width)[0].astype(BF16)

    outs = [
        jax.ShapeDtypeStruct((rows, LANES), F32),
        jax.ShapeDtypeStruct((rows, width), F32),
        jax.ShapeDtypeStruct((rows, heads * state), F32),
        jax.ShapeDtypeStruct((8, width), F32),
        jax.ShapeDtypeStruct((rows, model // CORES), BF16),
    ]
    operands = (residual, mixer_gain, step_proj, step_bias, log_rate, skip_gain)
    return local_kernel(body, "head_terms", outs, operands, 2 * rows * model * total)


def silu(values):
    return values * jax.nn.sigmoid(values)


def mix(partials, scale, step, decay, skip, conv_old, conv_last, ssm_state, group_gain, out_proj):
    rows, heads, head_dim, state = ssm_state.shape
    width = heads * head_dim
    model = out_proj.shape[1]
    groups = width // state
    count = len(partials)

    def body(*refs):
        parts = refs[:count]
        (scale_ref, step_ref, decay_ref, skip_ref, old_ref, last_ref, state_ref, gain_ref, out_ref) = refs[
            count : count + 9
        ]
        proj_out, fed_out, write_out, mine_out, other_out, read_buf, sum_buf = refs[count + 9 :]
        rank = lax.axis_index("tp")
        summed = parts[0][...].astype(F32)
        for part in parts[1:]:
            summed = summed + part[...].astype(F32)
        projected = (summed * scale_ref[:, :1]).astype(BF16)
        proj_out[...] = projected
        fresh = projected.astype(F32)
        act = [
            silu(old_ref[j] + fresh[:, (j + 1) * width : (j + 2) * width] * last_ref[j : j + 1, :])
            for j in range(3)
        ]
        x_act, b_act, c_act = act
        fed = step_ref[...] * x_act
        fed_out[...] = fed
        write_out[...] = b_act
        c_low = c_act.astype(BF16)
        read_buf[...] = c_low.astype(F32)
        lane = lax.broadcasted_iota(jnp.int32, (1, width), 1)
        for s in range(rows):
            block = state_ref[s].reshape(width, state).astype(BF16)
            reads = [read_buf[s : s + 1, g * state : (g + 1) * state] for g in range(groups)]
            reads = jnp.concatenate(reads + [jnp.zeros((8 - groups, state), F32)], 0).astype(BF16)
            found = lax.dot_general(
                reads, block, (((1,), (1,)), ((), ())), preferred_element_type=F32
            )
            row = found[0:1]
            for g in range(1, groups):
                row = jnp.where(lane >= g * state, found[g : g + 1], row)
            sum_buf[s : s + 1, :] = row
        old_part = sum_buf[...]
        decay_ch = jnp.concatenate(
            [decay_ref[:, h * state : h * state + head_dim] for h in range(heads)], 1
        )
        both = []
        for g in range(groups):
            cols = slice(g * state, (g + 1) * state)
            inner = jnp.sum(b_act[:, cols] * c_act[:, cols], axis=-1, keepdims=True)
            both.append(fed[:, cols] * inner)
        ssm_out = decay_ch * old_part + jnp.concatenate(both, 1) + skip_ref[0:1] * x_act
        gated = ssm_out * silu(fresh[:, :width])
        start = pl.multiple_of(rank * width, LANES)
        gain = gain_ref[:, pl.ds(start, width)]
        mixed = []
        for g in range(groups):
            cols = slice(g * state, (g + 1) * state)
            mixed.append(gated[:, cols] * row_scale(gated[:, cols]) * gain[:, cols])
        mixed = jnp.concatenate(mixed, 1).astype(BF16)
        result = jnp.dot(mixed, out_ref[...], preferred_element_type=F32)
        mine, other = halves(result, rank % CORES, width)
        mine_out[...] = mine
        other_out[...] = other.astype(BF16)

    outs = [
        jax.ShapeDtypeStruct((rows, partials[0].shape[1]), BF16),
        jax.ShapeDtypeStruct((rows, width), F32),
        jax.ShapeDtypeStruct((rows, width), F32),
        jax.ShapeDtypeStruct((rows, model // CORES), F32),
        jax.ShapeDtypeStruct((rows, model // CORES), BF16),
    ]
    operands = (
        *partials, scale, step, decay, skip, conv_old, conv_last, ssm_state, group_gain, out_proj,
    )
    scratch = [pltpu.VMEM((rows, width), F32), pltpu.VMEM((rows, width), F32)]
    return local_kernel(body, "mix", outs, operands, 2 * rows * width * model, scratch)


def advance_state(ssm_state, decay, fed, written):
    rows, heads, head_dim, state = ssm_state.shape
    width = heads * head_dim
    groups = width // state
    per_group = heads // groups
    chunk = 8

    def body(state_ref, decay_ref, fed_ref, write_ref, out_ref):
        fed_cols = fed_ref[...].T
        for s in range(chunk):
            for h in range(heads):
                g = h // per_group
                fade = decay_ref[s : s + 1, h * state : (h + 1) * state]
                write = write_ref[s : s + 1, g * state : (g + 1) * state]
                column = fed_cols[h * head_dim : (h + 1) * head_dim, s : s + 1]
                out_ref[s, h] = fade * state_ref[s, h] + column * write

    block = pl.BlockSpec((chunk, heads, head_dim, state), lambda i: (i, 0, 0, 0))
    return pl.pallas_call(
        body,
        name="advance_state",
        grid=(rows // chunk,),
        out_shape=jax.ShapeDtypeStruct(ssm_state.shape, F32),
        in_specs=[
            block,
            pl.BlockSpec((chunk, heads * state), lambda i: (i, 0)),
            pl.BlockSpec((chunk, width), lambda i: (i, 0)),
            pl.BlockSpec((chunk, width), lambda i: (i, 0)),
        ],
        out_specs=block,
        cost_estimate=pl.CostEstimate(
            flops=8 << 20, bytes_accessed=2 * ssm_state.size * 4, transcendentals=0
        ),
    )(ssm_state, decay, fed, written)


def dense_branch(mine, other, ffn_gain, gate, up, down, blend):
    rows, half = mine.shape
    model = half * CORES
    width = model // lax.axis_size("tp")

    def body(mine_ref, other_ref, gain_ref, gate_ref, up_ref, down_ref, blend_ref, mine_out, other_out):
        core = lax.axis_index("tp") % CORES
        values = interleave(mine_ref[...].astype(F32), other_ref[...].astype(F32), core, width)
        normed = (values * row_scale(values) * gain_ref[...]).astype(BF16)
        gated = jnp.dot(normed, gate_ref[...], preferred_element_type=F32)
        raised = jnp.dot(normed, up_ref[...], preferred_element_type=F32)
        hidden = (silu(gated) * raised).astype(BF16)
        weight = jax.nn.sigmoid(
            jnp.sum(normed.astype(F32) * blend_ref[...].astype(F32), axis=-1, keepdims=True)
        )
        result = jnp.dot(hidden, down_ref[...], preferred_element_type=F32) * weight
        kept, sent = halves(result, core, width)
        mine_out[...] = kept
        other_out[...] = sent

    outs = [jax.ShapeDtypeStruct((rows, half), F32)] * 2
    operands = (mine, other, ffn_gain, gate, up, down, blend)
    return local_kernel(body, "dense_branch", outs, operands, 6 * rows * model * gate.shape[1])


def run_experts(tokens, ffn_gain, gate, up, down, dense_mine, dense_other, packed, depth):
    own, rest, own_other, rest_other = tokens
    rows, half = own.shape
    every = rows + rest.shape[0]
    model = half * CORES
    width = model // lax.axis_size("tp")
    experts = gate.shape[0]
    total = experts * lax.axis_size("ep")
    count = len(packed)

    def body(own_ref, rest_ref, own2_ref, rest2_ref, gain_ref, gate_ref, up_ref, down_ref, dm, do, *more):
        packed_refs, (mine_out, other_out) = more[:count], more[count:]
        core = lax.axis_index("tp") % CORES
        first = lax.axis_index("ep") * experts
        mine = jnp.concatenate([own_ref[...].astype(F32), rest_ref[...].astype(F32)], 0)
        other = jnp.concatenate([own2_ref[...].astype(F32), rest2_ref[...].astype(F32)], 0)
        values = interleave(mine, other, core, width)
        normed = (values * row_scale(values) * gain_ref[...]).astype(BF16)
        weights = jnp.concatenate([r[:, depth:].astype(F32) for r in packed_refs], 0)
        lane = lax.broadcasted_iota(jnp.int32, weights.shape, 1)
        result = None
        for j in range(experts):
            gated = jnp.dot(normed, gate_ref[j], preferred_element_type=F32)
            raised = jnp.dot(normed, up_ref[j], preferred_element_type=F32)
            picked = (lane == first + j) | (lane == first + j + total)
            share = jnp.sum(jnp.where(picked, weights, 0.0), axis=-1, keepdims=True)
            hidden = (silu(gated) * raised * share).astype(BF16)
            part = jnp.dot(hidden, down_ref[j], preferred_element_type=F32)
            result = part if result is None else result + part
        kept, sent = halves(result, core, width)
        mine_out[:rows] = kept[:rows] + dm[...]
        mine_out[rows:] = kept[rows:]
        other_out[:rows] = (sent[:rows] + do[...]).astype(BF16)
        other_out[rows:] = sent[rows:].astype(BF16)

    outs = [jax.ShapeDtypeStruct((every, half), F32), jax.ShapeDtypeStruct((every, half), BF16)]
    operands = (*tokens, ffn_gain, gate, up, down, dense_mine, dense_other, *packed)
    flops = 6 * every * model * gate.shape[2] * experts
    return local_kernel(body, "run_experts", outs, operands, flops)


def on_device(
    residual,
    mixer_gain,
    gate_proj,
    input_proj,
    write_proj,
    read_proj,
    step_proj,
    conv_weight,
    step_bias,
    log_rate,
    skip_gain,
    group_gain,
    ssm_state,
    conv_state,
    out_proj,
    ffn_gain,
    routes,
    route_weight,
    expert_gate,
    expert_up,
    expert_down,
    dense_gate,
    dense_up,
    dense_down,
    blend_weight,
):
    rows = residual.shape[0]
    depth, width = gate_proj.shape
    heads = ssm_state.shape[1]
    ep_count, tp_count = lax.axis_size("ep"), lax.axis_size("tp")
    z_count = tp_count // CORES
    tp_rank = lax.axis_index("tp")
    z_rank = tp_rank // CORES
    ep_steps, z_steps = range(1, ep_count), range(1, z_count)
    expert_total = expert_gate.shape[0] * ep_count
    as_row = lambda vector: vector.reshape(1, -1)

    packed = pack_tokens(ep_count, expert_total, residual, as_row(mixer_gain), routes, route_weight)
    blocks = [packed[0]] + [send_ep(packed[k], ep_count, k) for k in ep_steps]
    partials = project(blocks, (gate_proj, input_proj, write_proj, read_proj))
    parts = [partials[0]] + [send_ep(partials[k], ep_count, k, back=True) for k in ep_steps]

    scale, step, decay, skip, resid_half = head_terms(
        residual, as_row(mixer_gain), step_proj, as_row(step_bias), as_row(log_rate),
        as_row(skip_gain), heads, width,
    )
    taps = lax.dynamic_slice_in_dim(conv_weight, tp_rank * width, width, 2)
    conv_old = jnp.sum(
        conv_state.astype(F32) * taps[None, :-1], axis=1
    ).transpose(1, 0, 2)

    projected, fed, written, mine, other = mix(
        parts, scale, step, decay, skip, conv_old, taps[-1], ssm_state, as_row(group_gain), out_proj
    )
    newest = projected[:, width:].reshape(rows, 1, 3, width)
    new_conv = jnp.concatenate((conv_state[:, 1:], newest), axis=1)

    mine = mine + send_core(other, tp_count).astype(F32)
    shared = mine.astype(BF16)
    for k in z_steps:
        mine = mine + send_z(shared, z_count, k).astype(F32)
    resid_mid = (resid_half.astype(F32) + mine).astype(BF16)
    new_state = advance_state(ssm_state, decay, fed, written)

    others = [send_ep(resid_mid, ep_count, k) for k in ep_steps]
    rest = jnp.concatenate(others, 0)
    own_other = send_core(resid_mid, tp_count)
    dense_mine, dense_other = dense_branch(
        resid_mid, own_other, as_row(ffn_gain), dense_gate, dense_up, dense_down, as_row(blend_weight)
    )
    rest_other = send_core(rest, tp_count)
    mine, other = run_experts(
        (resid_mid, rest, own_other, rest_other), as_row(ffn_gain), expert_gate, expert_up,
        expert_down, dense_mine, dense_other, blocks, depth,
    )
    mine = mine + send_core(other, tp_count).astype(F32)
    total = mine[:rows]
    low = mine.astype(BF16)
    for k in ep_steps:
        total = total + send_ep(low[k * rows : (k + 1) * rows], ep_count, k, back=True).astype(F32)
    piece = lambda array, z: lax.dynamic_slice_in_dim(array, z * width, width, 1)
    low = total.astype(BF16)
    result = piece(total, z_rank) + piece(resid_mid, z_rank).astype(F32)
    for k in z_steps:
        result = result + send_z(piece(low, partner(z_count, z_rank, k)), z_count, k).astype(F32)
    return result.astype(BF16), new_state, new_conv


def solution(mesh):
    return jax.shard_map(
        on_device,
        mesh=mesh,
        in_specs=(
            P("ep", None),
            P(),
            P("ep", "tp"),
            P("ep", "tp"),
            P("ep", "tp"),
            P("ep", "tp"),
            P(),
            P(),
            P(),
            P(),
            P(),
            P(),
            P("ep", "tp", None, None),
            P("ep", None, None, "tp"),
            P("tp", None),
            P(),
            P("ep", None),
            P("ep", None),
            P("ep", None, "tp"),
            P("ep", None, "tp"),
            P("ep", "tp", None),
            P(None, "tp"),
            P(None, "tp"),
            P("tp", None),
            P(),
        ),
        out_specs=(P("ep", "tp"), P("ep", "tp", None, None), P("ep", None, None, "tp")),
        check_vma=False,
    )
```

```python
import jax
import jax.numpy as jnp
from jax import lax
from jax.experimental import pallas as pl
from jax.experimental.pallas import tpu as pltpu
from jax.sharding import PartitionSpec as P


epsilon = 1e-06
CORES = 2
LANES = 128
F32 = jnp.float32
BF16 = jnp.bfloat16
EXACT = lax.Precision.HIGHEST


def partner(count, index, step):
    return index ^ step if count & (count - 1) == 0 else (index + step) % count


def send_ep(block, count, step, back=False):
    pairs = [(i, partner(count, i, step)) for i in range(count)]
    return lax.ppermute(block, "ep", [(b, a) for a, b in pairs] if back else pairs)


def send_z(block, count, step):
    pairs = [
        (z * CORES + c, partner(count, z, step) * CORES + c)
        for z in range(count)
        for c in range(CORES)
    ]
    return lax.ppermute(block, "tp", pairs)


def send_core(block, count):
    return lax.ppermute(block, "tp", [(i, i ^ 1) for i in range(count)])


def local_kernel(body, outs, operands, flops=0, scratch=(), remote=(), far_outs=()):
    near, far = pl.BlockSpec(memory_space=pltpu.VMEM), pl.BlockSpec(memory_space=pltpu.HBM)
    call = pl.pallas_call(
        body,
        out_shape=outs,
        in_specs=[far if i in remote else near for i in range(len(operands))],
        out_specs=[far if i in far_outs else near for i in range(len(outs))],
        scratch_shapes=scratch,
        cost_estimate=pl.CostEstimate(flops=flops, bytes_accessed=0, transcendentals=0),
        compiler_params=pltpu.CompilerParams(vmem_limit_bytes=40 << 20),
    )
    return call(
        *(
            pltpu.with_memory_space_constraint(x, pltpu.HBM) if i in remote else x
            for i, x in enumerate(operands)
        )
    )


def fetch(pairs, sems):
    copies = [pltpu.make_async_copy(a, b, sems.at[i]) for i, (a, b) in enumerate(pairs)]
    for copy in copies:
        copy.start()
    return copies


def row_scale(values):
    return lax.rsqrt(jnp.mean(values * values, axis=-1, keepdims=True) + epsilon)


def halves(array, core, width):
    count = array.shape[1] // width
    even = jnp.concatenate([array[:, i * width : (i + 1) * width] for i in range(0, count, 2)], 1)
    odd = jnp.concatenate([array[:, i * width : (i + 1) * width] for i in range(1, count, 2)], 1)
    first = core == 0
    return jnp.where(first, even, odd), jnp.where(first, odd, even)


def interleave(mine, other, core, width):
    first = core == 0
    even, odd = jnp.where(first, mine, other), jnp.where(first, other, mine)
    parts = []
    for i in range(mine.shape[1] // width):
        parts += [even[:, i * width : (i + 1) * width], odd[:, i * width : (i + 1) * width]]
    return jnp.concatenate(parts, 1)


def pack_tokens(ep_count, expert_total, residual, mixer_gain, routes, route_weight):
    rows, model = residual.shape
    choices = routes.shape[0]
    depth = model // ep_count
    side = -(-2 * expert_total // LANES) * LANES

    def body(res_hbm, gain_hbm, routes_hbm, weight_hbm, *refs):
        outs, (res_ref, gain_ref, routes_ref, weight_ref, sems) = refs[:ep_count], refs[ep_count:]
        copies = fetch(
            (
                (routes_hbm, routes_ref),
                (weight_hbm, weight_ref),
                (gain_hbm, gain_ref),
                (res_hbm, res_ref),
            ),
            sems,
        )
        for copy in copies:
            copy.wait()
        rank = lax.axis_index("ep")
        slot = lax.broadcasted_iota(jnp.int32, (side, rows), 0)
        named = jnp.where(slot < expert_total, slot, slot - expert_total)
        dense = jnp.zeros((side, rows), F32)
        for k in range(choices):
            dense = dense + jnp.where(
                routes_ref[k : k + 1, :] == named, weight_ref[k : k + 1, :], 0.0
            )
        high = dense.astype(BF16).astype(F32)
        dense = jnp.where(slot < expert_total, high, dense - high).T.astype(BF16)
        for step, out in enumerate(outs):
            start = pl.multiple_of(partner(ep_count, rank, step) * depth, LANES)
            cols = res_ref[:, pl.ds(start, depth)].astype(F32) * gain_ref[:, pl.ds(start, depth)]
            out[:, :depth] = cols.astype(BF16)
            out[:, depth:] = dense

    outs = [jax.ShapeDtypeStruct((rows, depth + side), BF16)] * ep_count
    operands = (residual, mixer_gain, routes, route_weight)
    scratch = [pltpu.VMEM(x.shape, x.dtype) for x in operands] + [pltpu.SemaphoreType.DMA((4,))]
    return local_kernel(body, outs, operands, 0, scratch, range(4))


def project(blocks, weights):
    rows = blocks[0].shape[0]
    depth, width = weights[0].shape
    count, kinds = len(blocks), len(weights)

    def body(*refs):
        ins, mats, outs = refs[:count], refs[count : count + kinds], refs[count + kinds :]
        stacked = jnp.concatenate([r[:, :depth] for r in ins], 0)
        for j, mat in enumerate(mats):
            result = jnp.dot(stacked, mat[...], preferred_element_type=F32)
            for i, out in enumerate(outs):
                piece = result[i * rows : (i + 1) * rows]
                out[:, j * width : (j + 1) * width] = piece.astype(out.dtype)

    outs = [jax.ShapeDtypeStruct((rows, kinds * width), BF16 if i else F32) for i in range(count)]
    flops = 2 * rows * count * depth * kinds * width
    return local_kernel(body, outs, (*blocks, *weights), flops)


def head_terms(residual, mixer_gain, step_proj, step_bias, log_rate, skip_gain, conv_state, conv_weight,
               group_gain, weights, heads, width):
    rows, model = residual.shape
    total = step_proj.shape[0]
    state = LANES
    kinds, taps = conv_weight.shape[:2]
    count = len(weights)
    fetched = (residual, mixer_gain, step_proj, step_bias, log_rate, skip_gain, conv_state)

    def body(*refs):
        sources, refs = refs[: len(fetched)], refs[len(fetched) :]
        tap_hbm, group_hbm, refs = refs[0], refs[1], refs[2:]
        weight_hbm, refs = refs[:count], refs[count:]
        (scale, step, decay, skip, half, old, last, gain_out), refs = refs[:8], refs[8:]
        weight_outs, refs = refs[:count], refs[count:]
        held, (tap_ref, sems) = refs[: len(fetched)], refs[len(fetched) :]
        res_ref, gain_ref, proj_ref, bias_ref, rate_ref, skip_ref, conv_ref = held
        rank = lax.axis_index("tp")
        mine = pl.ds(pl.multiple_of(rank * width, LANES), width)
        copies = fetch(
            (
                *zip(sources, held),
                (tap_hbm.at[:, :, mine], tap_ref),
                (group_hbm.at[:, mine], gain_out),
                *zip(weight_hbm, weight_outs),
            ),
            sems,
        )
        local = len(fetched) + 2
        for copy in copies[:local]:
            copy.wait()
        head_start = rank * heads
        values = res_ref[...].astype(F32)
        scaling = row_scale(values)
        normed = (values * scaling * gain_ref[...]).astype(BF16)
        raw = lax.dot_general(
            normed, proj_ref[...], (((1,), (1,)), ((), ())), preferred_element_type=F32
        )
        raw = raw + bias_ref[...]
        size = jnp.maximum(raw, 0.0) + jnp.log1p(jnp.exp(-jnp.abs(raw)))
        fade = jnp.exp(-jnp.exp(rate_ref[...]) * size)

        def spread(table, lanes):
            head = lax.broadcasted_iota(jnp.int32, (total, heads * lanes), 0) - head_start
            lane = lax.broadcasted_iota(jnp.int32, (total, heads * lanes), 1)
            hot = ((lane >= head * lanes) & (lane < (head + 1) * lanes)).astype(F32)
            return jnp.dot(table, hot, preferred_element_type=F32, precision=EXACT)

        scale[...] = jnp.broadcast_to(scaling, (rows, LANES))
        step[...] = spread(size, width // heads)
        decay[...] = spread(fade, state)
        skip[...] = spread(jnp.broadcast_to(skip_ref[...], (8, total)), width // heads)
        half[...] = halves(values, rank % CORES, width)[0].astype(BF16)
        for j in range(kinds):
            part = conv_ref[0, j].astype(F32) * tap_ref[j, 0:1]
            for k in range(1, taps - 1):
                part = part + conv_ref[k, j].astype(F32) * tap_ref[j, k : k + 1]
            old[j] = part
            last[j : j + 1, :] = tap_ref[j, taps - 1 : taps]
        for copy in copies[local:]:
            copy.wait()

    outs = [
        jax.ShapeDtypeStruct((rows, LANES), F32),
        jax.ShapeDtypeStruct((rows, width), F32),
        jax.ShapeDtypeStruct((rows, heads * state), F32),
        jax.ShapeDtypeStruct((8, width), F32),
        jax.ShapeDtypeStruct((rows, model // CORES), BF16),
        jax.ShapeDtypeStruct((kinds, rows, width), F32),
        jax.ShapeDtypeStruct((8, width), F32),
        jax.ShapeDtypeStruct((1, width), F32),
        *(jax.ShapeDtypeStruct(w.shape, w.dtype) for w in weights),
    ]
    operands = (*fetched, conv_weight, group_gain, *weights)
    scratch = [
        *(pltpu.VMEM(x.shape, x.dtype) for x in fetched),
        pltpu.VMEM((kinds, taps, width), F32),
        pltpu.SemaphoreType.DMA((len(operands),)),
    ]
    flops = 2 * rows * model * total
    return local_kernel(body, outs, operands, flops, scratch, range(len(operands)))


def load(arrays):
    count = len(arrays)

    def body(*refs):
        for copy in fetch(list(zip(refs[:count], refs[count : 2 * count])), refs[-1]):
            copy.wait()

    outs = [jax.ShapeDtypeStruct(x.shape, x.dtype) for x in arrays]
    scratch = [pltpu.SemaphoreType.DMA((count,))]
    return local_kernel(body, outs, arrays, 0, scratch, range(count))


def silu(values):
    return values * jax.nn.sigmoid(values)


def mix(partials, scale, step, decay, skip, conv_old, conv_last, ssm_state, group_gain, out_proj):
    rows, heads, head_dim, state = ssm_state.shape
    width = heads * head_dim
    model = out_proj.shape[1]
    groups = width // state
    count = len(partials)

    def body(*refs):
        parts = refs[:count]
        (scale_ref, step_ref, decay_ref, skip_ref, old_ref, last_ref, state_ref, gain_ref, out_ref) = refs[
            count : count + 9
        ]
        proj_out, fed_out, write_out, mine_out, other_out, read_buf, sum_buf = refs[count + 9 :]
        rank = lax.axis_index("tp")
        summed = parts[0][...].astype(F32)
        for part in parts[1:]:
            summed = summed + part[...].astype(F32)
        projected = (summed * scale_ref[:, :1]).astype(BF16)
        proj_out[...] = projected
        fresh = projected.astype(F32)
        act = [
            silu(old_ref[j] + fresh[:, (j + 1) * width : (j + 2) * width] * last_ref[j : j + 1, :])
            for j in range(3)
        ]
        x_act, b_act, c_act = act
        fed = step_ref[...] * x_act
        fed_out[...] = fed
        write_out[...] = b_act
        c_low = c_act.astype(BF16)
        read_buf[...] = c_low.astype(F32)
        lane = lax.broadcasted_iota(jnp.int32, (1, width), 1)
        for s in range(rows):
            block = state_ref[s].reshape(width, state).astype(BF16)
            reads = [read_buf[s : s + 1, g * state : (g + 1) * state] for g in range(groups)]
            reads = jnp.concatenate(reads + [jnp.zeros((8 - groups, state), F32)], 0).astype(BF16)
            found = lax.dot_general(
                reads, block, (((1,), (1,)), ((), ())), preferred_element_type=F32
            )
            row = found[0:1]
            for g in range(1, groups):
                row = jnp.where(lane >= g * state, found[g : g + 1], row)
            sum_buf[s : s + 1, :] = row
        old_part = sum_buf[...]
        decay_ch = jnp.concatenate(
            [decay_ref[:, h * state : h * state + head_dim] for h in range(heads)], 1
        )
        both = []
        for g in range(groups):
            cols = slice(g * state, (g + 1) * state)
            inner = jnp.sum(b_act[:, cols] * c_act[:, cols], axis=-1, keepdims=True)
            both.append(fed[:, cols] * inner)
        ssm_out = decay_ch * old_part + jnp.concatenate(both, 1) + skip_ref[0:1] * x_act
        gated = ssm_out * silu(fresh[:, :width])
        gain = gain_ref[...]
        mixed = []
        for g in range(groups):
            cols = slice(g * state, (g + 1) * state)
            mixed.append(gated[:, cols] * row_scale(gated[:, cols]) * gain[:, cols])
        mixed = jnp.concatenate(mixed, 1).astype(BF16)
        result = jnp.dot(mixed, out_ref[...], preferred_element_type=F32)
        mine, other = halves(result, rank % CORES, width)
        mine_out[...] = mine
        other_out[...] = other.astype(BF16)

    outs = [
        jax.ShapeDtypeStruct((rows, partials[0].shape[1]), BF16),
        jax.ShapeDtypeStruct((rows, width), F32),
        jax.ShapeDtypeStruct((rows, width), F32),
        jax.ShapeDtypeStruct((rows, model // CORES), F32),
        jax.ShapeDtypeStruct((rows, model // CORES), BF16),
    ]
    operands = (
        *partials, scale, step, decay, skip, conv_old, conv_last, ssm_state, group_gain, out_proj,
    )
    scratch = [pltpu.VMEM((rows, width), F32), pltpu.VMEM((rows, width), F32)]
    return local_kernel(body, outs, operands, 2 * rows * width * model, scratch)


def advance_state(ssm_state, decay, fed, written, projected, conv_state):
    rows, heads, head_dim, state = ssm_state.shape
    width = heads * head_dim
    groups = width // state
    per_group = heads // groups
    taps, kinds = conv_state.shape[:2]
    chunk = 8

    def body(state_ref, decay_ref, fed_ref, write_ref, proj_ref, conv_hbm, out_hbm, conv_out, *scratch):
        buf, fresh, sems = scratch
        shift = pltpu.make_async_copy(
            conv_hbm.at[1:], conv_out.at[: taps - 1], sems.at[rows // chunk]
        )
        shift.start()
        for j in range(kinds):
            fresh[j] = proj_ref[:, (j + 1) * width : (j + 2) * width]
        newest = pltpu.make_async_copy(fresh, conv_out.at[taps - 1], sems.at[rows // chunk + 1])
        newest.start()
        fed_cols = fed_ref[...].T
        copies = [shift, newest]
        for s in range(rows):
            for h in range(heads):
                g = h // per_group
                fade = decay_ref[s : s + 1, h * state : (h + 1) * state]
                write = write_ref[s : s + 1, g * state : (g + 1) * state]
                column = fed_cols[h * head_dim : (h + 1) * head_dim, s : s + 1]
                buf[s, h] = fade * state_ref[s, h] + column * write
            if s % chunk == chunk - 1:
                span = pl.ds(s - chunk + 1, chunk)
                done = pltpu.make_async_copy(buf.at[span], out_hbm.at[span], sems.at[s // chunk])
                done.start()
                copies.append(done)
        for copy in copies:
            copy.wait()

    outs = [
        jax.ShapeDtypeStruct(ssm_state.shape, F32),
        jax.ShapeDtypeStruct(conv_state.shape, conv_state.dtype),
    ]
    scratch = [
        pltpu.VMEM(ssm_state.shape, F32),
        pltpu.VMEM((kinds, rows, width), conv_state.dtype),
        pltpu.SemaphoreType.DMA((rows // chunk + 2,)),
    ]
    operands = (ssm_state, decay, fed, written, projected, conv_state)
    return local_kernel(body, outs, operands, 8 << 20, scratch, (5,), (0, 1))


def dense_branch(mine, other, ffn_gain, gate, up, down, blend):
    rows, half = mine.shape
    model = half * CORES
    width = model // lax.axis_size("tp")

    def body(mine_ref, other_ref, gain_ref, gate_ref, up_ref, down_ref, blend_ref, mine_out, other_out):
        core = lax.axis_index("tp") % CORES
        values = interleave(mine_ref[...].astype(F32), other_ref[...].astype(F32), core, width)
        normed = (values * row_scale(values) * gain_ref[...]).astype(BF16)
        gated = jnp.dot(normed, gate_ref[...], preferred_element_type=F32)
        raised = jnp.dot(normed, up_ref[...], preferred_element_type=F32)
        hidden = (silu(gated) * raised).astype(BF16)
        weight = jax.nn.sigmoid(
            jnp.sum(normed.astype(F32) * blend_ref[...].astype(F32), axis=-1, keepdims=True)
        )
        result = jnp.dot(hidden, down_ref[...], preferred_element_type=F32) * weight
        kept, sent = halves(result, core, width)
        mine_out[...] = kept
        other_out[...] = sent

    outs = [jax.ShapeDtypeStruct((rows, half), F32)] * 2
    operands = (mine, other, ffn_gain, gate, up, down, blend)
    return local_kernel(body, outs, operands, 6 * rows * model * gate.shape[1])


def run_experts(tokens, ffn_gain, gate, up, down, dense_mine, dense_other, packed, depth):
    own, rest, _, _ = tokens
    rows, half = own.shape
    every = rows + rest.shape[0]
    model = half * CORES
    width = model // lax.axis_size("tp")
    experts = gate.shape[0]
    total = experts * lax.axis_size("ep")
    count = len(packed)

    def body(own_ref, rest_ref, own2_ref, rest2_ref, gain_ref, gate_ref, up_ref, down_ref, dm, do, *more):
        packed_refs, (mine_out, other_out) = more[:count], more[count:]
        core = lax.axis_index("tp") % CORES
        first = lax.axis_index("ep") * experts
        mine = jnp.concatenate([own_ref[...].astype(F32), rest_ref[...].astype(F32)], 0)
        other = jnp.concatenate([own2_ref[...].astype(F32), rest2_ref[...].astype(F32)], 0)
        values = interleave(mine, other, core, width)
        normed = (values * row_scale(values) * gain_ref[...]).astype(BF16)
        weights = jnp.concatenate([r[:, depth:].astype(F32) for r in packed_refs], 0)
        lane = lax.broadcasted_iota(jnp.int32, weights.shape, 1)
        result = None
        for j in range(experts):
            gated = jnp.dot(normed, gate_ref[j], preferred_element_type=F32)
            raised = jnp.dot(normed, up_ref[j], preferred_element_type=F32)
            picked = (lane == first + j) | (lane == first + j + total)
            share = jnp.sum(jnp.where(picked, weights, 0.0), axis=-1, keepdims=True)
            hidden = (silu(gated) * raised * share).astype(BF16)
            part = jnp.dot(hidden, down_ref[j], preferred_element_type=F32)
            result = part if result is None else result + part
        kept, sent = halves(result, core, width)
        mine_out[:rows] = kept[:rows] + dm[...]
        mine_out[rows:] = kept[rows:]
        other_out[:rows] = (sent[:rows] + do[...]).astype(BF16)
        other_out[rows:] = sent[rows:].astype(BF16)

    outs = [jax.ShapeDtypeStruct((every, half), F32), jax.ShapeDtypeStruct((every, half), BF16)]
    operands = (*tokens, ffn_gain, gate, up, down, dense_mine, dense_other, *packed)
    flops = 6 * every * model * gate.shape[2] * experts
    return local_kernel(body, outs, operands, flops)


def layer(
    residual,
    mixer_gain,
    gate_proj,
    input_proj,
    write_proj,
    read_proj,
    step_proj,
    conv_weight,
    step_bias,
    log_rate,
    skip_gain,
    group_gain,
    ssm_state,
    conv_state,
    out_proj,
    ffn_gain,
    routes,
    route_weight,
    expert_gate,
    expert_up,
    expert_down,
    dense_gate,
    dense_up,
    dense_down,
    blend_weight,
):
    rows = residual.shape[0]
    depth, width = gate_proj.shape
    heads = ssm_state.shape[1]
    ep_count, tp_count = lax.axis_size("ep"), lax.axis_size("tp")
    z_count = tp_count // CORES
    tp_rank = lax.axis_index("tp")
    z_rank = tp_rank // CORES
    ep_steps, z_steps = range(1, ep_count), range(1, z_count)
    expert_total = expert_gate.shape[0] * ep_count
    as_row = lambda vector: vector.reshape(1, -1)

    packed = pack_tokens(
        ep_count, expert_total, residual, as_row(mixer_gain), routes.T, route_weight.T
    )
    blocks = [packed[0]] + [send_ep(packed[k], ep_count, k) for k in ep_steps]
    conv_rows = conv_state.transpose(1, 2, 0, 3)
    scale, step, decay, skip, resid_half, conv_old, conv_last, gain, *weights = head_terms(
        residual, as_row(mixer_gain), step_proj.T, as_row(step_bias), as_row(log_rate),
        as_row(skip_gain), conv_rows, conv_weight.transpose(1, 0, 2), as_row(group_gain),
        (gate_proj, input_proj, write_proj, read_proj), heads, width,
    )
    partials = project(blocks, weights)
    parts = [partials[0]] + [send_ep(partials[k], ep_count, k, back=True) for k in ep_steps]
    state, out_weight = load((ssm_state, out_proj))
    projected, fed, written, mine, other = mix(
        parts, scale, step, decay, skip, conv_old, conv_last, state, gain, out_weight
    )

    mine = mine + send_core(other, tp_count).astype(F32)
    shared = mine.astype(BF16)
    gathered = [send_z(shared, z_count, k) for k in z_steps]
    new_state, new_conv = advance_state(state, decay, fed, written, projected, conv_rows)
    new_conv = new_conv.transpose(2, 0, 1, 3)
    for part in gathered:
        mine = mine + part.astype(F32)
    resid_mid = (resid_half.astype(F32) + mine).astype(BF16)

    others = [send_ep(resid_mid, ep_count, k) for k in ep_steps]
    own_other = send_core(resid_mid, tp_count)
    dense_mine, dense_other = dense_branch(
        resid_mid, own_other, as_row(ffn_gain), dense_gate, dense_up, dense_down, as_row(blend_weight)
    )
    rest = jnp.concatenate(others, 0)
    rest_other = send_core(rest, tp_count)
    mine, other = run_experts(
        (resid_mid, rest, own_other, rest_other), as_row(ffn_gain), expert_gate, expert_up,
        expert_down, dense_mine, dense_other, blocks, depth,
    )
    mine = mine + send_core(other, tp_count).astype(F32)
    total = mine[:rows]
    low = mine.astype(BF16)
    for k in ep_steps:
        total = total + send_ep(low[k * rows : (k + 1) * rows], ep_count, k, back=True).astype(F32)
    piece = lambda array, z: lax.dynamic_slice_in_dim(array, z * width, width, 1)
    low = total.astype(BF16)
    result = piece(total, z_rank) + piece(resid_mid, z_rank).astype(F32)
    for k in z_steps:
        result = result + send_z(piece(low, partner(z_count, z_rank, k)), z_count, k).astype(F32)
    return result.astype(BF16), new_state, new_conv


def solution(mesh):
    return jax.shard_map(
        layer,
        mesh=mesh,
        in_specs=(
            P("ep", None),
            P(),
            P("ep", "tp"),
            P("ep", "tp"),
            P("ep", "tp"),
            P("ep", "tp"),
            P(),
            P(),
            P(),
            P(),
            P(),
            P(),
            P("ep", "tp", None, None),
            P("ep", None, None, "tp"),
            P("tp", None),
            P(),
            P("ep", None),
            P("ep", None),
            P("ep", None, "tp"),
            P("ep", None, "tp"),
            P("ep", "tp", None),
            P(None, "tp"),
            P(None, "tp"),
            P("tp", None),
            P(),
        ),
        out_specs=(P("ep", "tp"), P("ep", "tp", None, None), P("ep", None, None, "tp")),
        check_vma=False,
    )
```

```python
import jax
import jax.numpy as jnp
from jax import lax
from jax.experimental import pallas as pl
from jax.experimental.pallas import tpu as pltpu
from jax.sharding import PartitionSpec as P


epsilon = 1e-06
CORES = 2
LANES = 128
F32 = jnp.float32
BF16 = jnp.bfloat16
EXACT = lax.Precision.HIGHEST


def partner(count, index, step):
    return index ^ step if count & (count - 1) == 0 else (index + step) % count


def hop(block, pairs):
    return lax.ppermute(block, ("ep", "tp"), pairs)


def send_ep(block, ep_count, tp_count, step, cross=False, back=False):
    pairs = [
        (i * tp_count + t, partner(ep_count, i, step) * tp_count + (t ^ cross))
        for i in range(ep_count)
        for t in range(tp_count)
    ]
    return hop(block, [(b, a) for a, b in pairs] if back else pairs)


def send_z(block, ep_count, tp_count, step, cross=False):
    z_count = tp_count // CORES
    pairs = [
        (i * tp_count + z * CORES + c, i * tp_count + partner(z_count, z, step) * CORES + (c ^ cross))
        for i in range(ep_count)
        for z in range(z_count)
        for c in range(CORES)
    ]
    return hop(block, pairs)


def send_core(block, count):
    return lax.ppermute(block, "tp", [(i, i ^ 1) for i in range(count)])


def local_kernel(body, outs, operands, flops=0, scratch=(), remote=(), far_outs=()):
    near, far = pl.BlockSpec(memory_space=pltpu.VMEM), pl.BlockSpec(memory_space=pltpu.HBM)
    call = pl.pallas_call(
        body,
        out_shape=outs,
        in_specs=[far if i in remote else near for i in range(len(operands))],
        out_specs=[far if i in far_outs else near for i in range(len(outs))],
        scratch_shapes=scratch,
        cost_estimate=pl.CostEstimate(flops=flops, bytes_accessed=0, transcendentals=0),
        compiler_params=pltpu.CompilerParams(vmem_limit_bytes=40 << 20),
    )
    return call(
        *(
            pltpu.with_memory_space_constraint(x, pltpu.HBM) if i in remote else x
            for i, x in enumerate(operands)
        )
    )


def fetch(pairs, sems):
    copies = [pltpu.make_async_copy(a, b, sems.at[i]) for i, (a, b) in enumerate(pairs)]
    for copy in copies:
        copy.start()
    return copies


def row_scale(values):
    return lax.rsqrt(jnp.mean(values * values, axis=-1, keepdims=True) + epsilon)


def halves(array, core, width):
    count = array.shape[1] // width
    even = jnp.concatenate([array[:, i * width : (i + 1) * width] for i in range(0, count, 2)], 1)
    odd = jnp.concatenate([array[:, i * width : (i + 1) * width] for i in range(1, count, 2)], 1)
    first = core == 0
    return jnp.where(first, even, odd), jnp.where(first, odd, even)


def interleave(mine, other, core, width):
    first = core == 0
    even, odd = jnp.where(first, mine, other), jnp.where(first, other, mine)
    parts = []
    for i in range(mine.shape[1] // width):
        parts += [even[:, i * width : (i + 1) * width], odd[:, i * width : (i + 1) * width]]
    return jnp.concatenate(parts, 1)


def project(blocks, gain, weights):
    rows = blocks[0].shape[0]
    depth, width = weights[0].shape
    count, kinds = len(blocks), len(weights)

    def body(*refs):
        ins, gain_ref, refs = refs[:count], refs[count], refs[count + 1 :]
        mats, outs = refs[:kinds], refs[kinds:]
        scaled = [(r[...].astype(F32) * gain_ref[...]).astype(BF16) for r in ins]
        stacked = jnp.concatenate(scaled, 0)
        for j, mat in enumerate(mats):
            result = jnp.dot(stacked, mat[...], preferred_element_type=F32)
            for i, out in enumerate(outs):
                piece = result[i * rows : (i + 1) * rows]
                out[:, j * width : (j + 1) * width] = piece.astype(out.dtype)

    outs = [jax.ShapeDtypeStruct((rows, kinds * width), BF16 if i else F32) for i in range(count)]
    flops = 2 * rows * count * depth * kinds * width
    return local_kernel(body, outs, (*blocks, gain, *weights), flops)


def head_terms(
    residual, mixer_gain, step_proj, step_bias, log_rate, skip_gain, conv_state, routes, route_weight,
    conv_weight, group_gain, weights, heads, width, expert_total,
):
    rows, model = residual.shape
    total = step_proj.shape[0]
    state = LANES
    kinds, taps = conv_weight.shape[:2]
    count = len(weights)
    depth = weights[0].shape[0]
    side = -(-2 * expert_total // LANES) * LANES
    fetched = (
        residual, mixer_gain, step_proj, step_bias, log_rate, skip_gain, conv_state, routes, route_weight,
    )

    def body(*refs):
        sources, refs = refs[: len(fetched)], refs[len(fetched) :]
        tap_hbm, group_hbm, refs = refs[0], refs[1], refs[2:]
        weight_hbm, refs = refs[:count], refs[count:]
        (scale, step, decay, skip, half, old, last, gain_out), refs = refs[:8], refs[8:]
        (own_out, depth_gain, table_out), refs = refs[:3], refs[3:]
        weight_outs, refs = refs[:count], refs[count:]
        held, (tap_ref, sems) = refs[: len(fetched)], refs[len(fetched) :]
        res_ref, gain_ref, proj_ref, bias_ref, rate_ref, skip_ref, conv_ref, routes_ref, share_ref = held
        rank = lax.axis_index("tp")
        mine = pl.ds(pl.multiple_of(rank * width, LANES), width)
        copies = fetch(
            (
                *zip(sources, held),
                (tap_hbm.at[:, :, mine], tap_ref),
                (group_hbm.at[:, mine], gain_out),
                *zip(weight_hbm, weight_outs),
            ),
            sems,
        )
        local = len(fetched) + 2
        for copy in copies[:local]:
            copy.wait()
        head_start = rank * heads
        values = res_ref[...].astype(F32)
        scaling = row_scale(values)
        normed = (values * scaling * gain_ref[...]).astype(BF16)
        raw = lax.dot_general(
            normed, proj_ref[...], (((1,), (1,)), ((), ())), preferred_element_type=F32
        )
        raw = raw + bias_ref[...]
        size = jnp.maximum(raw, 0.0) + jnp.log1p(jnp.exp(-jnp.abs(raw)))
        fade = jnp.exp(-jnp.exp(rate_ref[...]) * size)

        def spread(table, lanes):
            head = lax.broadcasted_iota(jnp.int32, (total, heads * lanes), 0) - head_start
            lane = lax.broadcasted_iota(jnp.int32, (total, heads * lanes), 1)
            hot = ((lane >= head * lanes) & (lane < (head + 1) * lanes)).astype(F32)
            return jnp.dot(table, hot, preferred_element_type=F32, precision=EXACT)

        scale[...] = jnp.broadcast_to(scaling, (rows, LANES))
        step[...] = spread(size, width // heads)
        decay[...] = spread(fade, state)
        skip[...] = spread(jnp.broadcast_to(skip_ref[...], (8, total)), width // heads)
        half[...] = halves(values, rank % CORES, width)[0].astype(BF16)
        for j in range(kinds):
            part = conv_ref[0, j].astype(F32) * tap_ref[j, 0:1]
            for k in range(1, taps - 1):
                part = part + conv_ref[k, j].astype(F32) * tap_ref[j, k : k + 1]
            old[j] = part
            last[j : j + 1, :] = tap_ref[j, taps - 1 : taps]
        owned = pl.ds(pl.multiple_of(lax.axis_index("ep") * depth, LANES), depth)
        own_out[...] = res_ref[:, owned]
        depth_gain[...] = gain_ref[:, owned]
        slot = lax.broadcasted_iota(jnp.int32, (side, rows), 0)
        named = jnp.where(slot < expert_total, slot, slot - expert_total)
        table = jnp.zeros((side, rows), F32)
        for k in range(routes.shape[0]):
            table = table + jnp.where(
                routes_ref[k : k + 1, :] == named, share_ref[k : k + 1, :], 0.0
            )
        high = table.astype(BF16).astype(F32)
        table_out[...] = jnp.where(slot < expert_total, high, table - high).T.astype(BF16)
        for copy in copies[local:]:
            copy.wait()

    outs = [
        jax.ShapeDtypeStruct((rows, LANES), F32),
        jax.ShapeDtypeStruct((rows, width), F32),
        jax.ShapeDtypeStruct((rows, heads * state), F32),
        jax.ShapeDtypeStruct((8, width), F32),
        jax.ShapeDtypeStruct((rows, model // CORES), BF16),
        jax.ShapeDtypeStruct((kinds, rows, width), F32),
        jax.ShapeDtypeStruct((8, width), F32),
        jax.ShapeDtypeStruct((1, width), F32),
        jax.ShapeDtypeStruct((rows, depth), BF16),
        jax.ShapeDtypeStruct((1, depth), F32),
        jax.ShapeDtypeStruct((rows, side), BF16),
        *(jax.ShapeDtypeStruct(w.shape, w.dtype) for w in weights),
    ]
    operands = (*fetched, conv_weight, group_gain, *weights)
    scratch = [
        *(pltpu.VMEM(x.shape, x.dtype) for x in fetched),
        pltpu.VMEM((kinds, taps, width), F32),
        pltpu.SemaphoreType.DMA((len(operands),)),
    ]
    flops = 2 * rows * model * total
    return local_kernel(body, outs, operands, flops, scratch, range(len(operands)))


def load(arrays):
    count = len(arrays)

    def body(*refs):
        for copy in fetch(list(zip(refs[:count], refs[count : 2 * count])), refs[-1]):
            copy.wait()

    outs = [jax.ShapeDtypeStruct(x.shape, x.dtype) for x in arrays]
    scratch = [pltpu.SemaphoreType.DMA((count,))]
    return local_kernel(body, outs, arrays, 0, scratch, range(count))


def silu(values):
    return values * jax.nn.sigmoid(values)


def mix(partials, scale, step, decay, skip, conv_old, conv_last, ssm_state, group_gain, out_proj):
    rows, heads, head_dim, state = ssm_state.shape
    width = heads * head_dim
    model = out_proj.shape[1]
    groups = width // state
    count = len(partials)

    def body(*refs):
        parts = refs[:count]
        (scale_ref, step_ref, decay_ref, skip_ref, old_ref, last_ref, state_ref, gain_ref, out_ref) = refs[
            count : count + 9
        ]
        proj_out, fed_out, write_out, mine_out, other_out, read_buf, sum_buf = refs[count + 9 :]
        rank = lax.axis_index("tp")
        summed = parts[0][...].astype(F32)
        for part in parts[1:]:
            summed = summed + part[...].astype(F32)
        projected = (summed * scale_ref[:, :1]).astype(BF16)
        proj_out[...] = projected
        fresh = projected.astype(F32)
        act = [
            silu(old_ref[j] + fresh[:, (j + 1) * width : (j + 2) * width] * last_ref[j : j + 1, :])
            for j in range(3)
        ]
        x_act, b_act, c_act = act
        fed = step_ref[...] * x_act
        fed_out[...] = fed
        write_out[...] = b_act
        c_low = c_act.astype(BF16)
        read_buf[...] = c_low.astype(F32)
        lane = lax.broadcasted_iota(jnp.int32, (1, width), 1)
        for s in range(rows):
            block = state_ref[s].reshape(width, state).astype(BF16)
            reads = [read_buf[s : s + 1, g * state : (g + 1) * state] for g in range(groups)]
            reads = jnp.concatenate(reads + [jnp.zeros((8 - groups, state), F32)], 0).astype(BF16)
            found = lax.dot_general(
                reads, block, (((1,), (1,)), ((), ())), preferred_element_type=F32
            )
            row = found[0:1]
            for g in range(1, groups):
                row = jnp.where(lane >= g * state, found[g : g + 1], row)
            sum_buf[s : s + 1, :] = row
        old_part = sum_buf[...]
        decay_ch = jnp.concatenate(
            [decay_ref[:, h * state : h * state + head_dim] for h in range(heads)], 1
        )
        both = []
        for g in range(groups):
            cols = slice(g * state, (g + 1) * state)
            inner = jnp.sum(b_act[:, cols] * c_act[:, cols], axis=-1, keepdims=True)
            both.append(fed[:, cols] * inner)
        ssm_out = decay_ch * old_part + jnp.concatenate(both, 1) + skip_ref[0:1] * x_act
        gated = ssm_out * silu(fresh[:, :width])
        gain = gain_ref[...]
        mixed = []
        for g in range(groups):
            cols = slice(g * state, (g + 1) * state)
            mixed.append(gated[:, cols] * row_scale(gated[:, cols]) * gain[:, cols])
        mixed = jnp.concatenate(mixed, 1).astype(BF16)
        result = jnp.dot(mixed, out_ref[...], preferred_element_type=F32)
        mine, other = halves(result, rank % CORES, width)
        mine_out[...] = mine
        other_out[...] = other.astype(BF16)

    outs = [
        jax.ShapeDtypeStruct((rows, partials[0].shape[1]), BF16),
        jax.ShapeDtypeStruct((rows, width), F32),
        jax.ShapeDtypeStruct((rows, width), F32),
        jax.ShapeDtypeStruct((rows, model // CORES), F32),
        jax.ShapeDtypeStruct((rows, model // CORES), BF16),
    ]
    operands = (
        *partials, scale, step, decay, skip, conv_old, conv_last, ssm_state, group_gain, out_proj,
    )
    scratch = [pltpu.VMEM((rows, width), F32), pltpu.VMEM((rows, width), F32)]
    return local_kernel(body, outs, operands, 2 * rows * width * model, scratch)


def advance_state(ssm_state, decay, fed, written, projected, conv_state):
    rows, heads, head_dim, state = ssm_state.shape
    width = heads * head_dim
    groups = width // state
    per_group = heads // groups
    taps, kinds = conv_state.shape[:2]
    chunk = 8

    def body(state_ref, decay_ref, fed_ref, write_ref, proj_ref, conv_hbm, out_hbm, conv_out, *scratch):
        buf, fresh, sems = scratch
        shift = pltpu.make_async_copy(
            conv_hbm.at[1:], conv_out.at[: taps - 1], sems.at[rows // chunk]
        )
        shift.start()
        for j in range(kinds):
            fresh[j] = proj_ref[:, (j + 1) * width : (j + 2) * width]
        newest = pltpu.make_async_copy(fresh, conv_out.at[taps - 1], sems.at[rows // chunk + 1])
        newest.start()
        fed_cols = fed_ref[...].T
        copies = [shift, newest]
        for s in range(rows):
            for h in range(heads):
                g = h // per_group
                fade = decay_ref[s : s + 1, h * state : (h + 1) * state]
                write = write_ref[s : s + 1, g * state : (g + 1) * state]
                column = fed_cols[h * head_dim : (h + 1) * head_dim, s : s + 1]
                buf[s, h] = fade * state_ref[s, h] + column * write
            if s % chunk == chunk - 1:
                span = pl.ds(s - chunk + 1, chunk)
                done = pltpu.make_async_copy(buf.at[span], out_hbm.at[span], sems.at[s // chunk])
                done.start()
                copies.append(done)
        for copy in copies:
            copy.wait()

    outs = [
        jax.ShapeDtypeStruct(ssm_state.shape, F32),
        jax.ShapeDtypeStruct(conv_state.shape, conv_state.dtype),
    ]
    scratch = [
        pltpu.VMEM(ssm_state.shape, F32),
        pltpu.VMEM((kinds, rows, width), conv_state.dtype),
        pltpu.SemaphoreType.DMA((rows // chunk + 2,)),
    ]
    operands = (ssm_state, decay, fed, written, projected, conv_state)
    return local_kernel(body, outs, operands, 8 << 20, scratch, (5,), (0, 1))


def column_blocks(width, z_count, kept):
    rank = lax.axis_index("tp")
    z, core = rank // CORES, rank % CORES
    starts = []
    for step in range(z_count):
        same = (step == 0) == kept
        parity = core if same else 1 - core
        starts.append(pl.multiple_of((partner(z_count, z, step) * CORES + parity) * width, LANES))
    return starts


def dense_branch(mine, other, ffn_gain, gate, up, down, blend):
    rows = mine.shape[0]
    model = gate.shape[0]
    half = model // CORES
    tp_count = lax.axis_size("tp")
    width = model // tp_count
    z_count = tp_count // CORES

    def body(mine_ref, other_ref, gain_ref, gate_ref, up_ref, down_ref, blend_ref, mine_out, other_out):
        core = lax.axis_index("tp") % CORES
        values = interleave(
            mine_ref[:, :half].astype(F32), other_ref[:, :half].astype(F32), core, width
        )
        normed = (values * row_scale(values) * gain_ref[...]).astype(BF16)
        gated = jnp.dot(normed, gate_ref[...], preferred_element_type=F32)
        raised = jnp.dot(normed, up_ref[...], preferred_element_type=F32)
        hidden = (silu(gated) * raised).astype(BF16)
        weight = jax.nn.sigmoid(
            jnp.sum(normed.astype(F32) * blend_ref[...].astype(F32), axis=-1, keepdims=True)
        )
        for kept, out in ((True, mine_out), (False, other_out)):
            for i, start in enumerate(column_blocks(width, z_count, kept)):
                part = jnp.dot(hidden, down_ref[:, pl.ds(start, width)], preferred_element_type=F32)
                out[:, i * width : (i + 1) * width] = part * weight

    outs = [jax.ShapeDtypeStruct((rows, half), F32)] * 2
    operands = (mine, other, ffn_gain, gate, up, down, blend)
    return local_kernel(body, outs, operands, 6 * rows * model * gate.shape[1])


def down_blocks(hidden, down_ref, width, z_count, kept):
    ffe = down_ref.shape[1]
    for i, start in enumerate(column_blocks(width, z_count, kept)):
        result = None
        for j in range(down_ref.shape[0]):
            part = jnp.dot(
                hidden[:, j * ffe : (j + 1) * ffe],
                down_ref[j, :, pl.ds(start, width)],
                preferred_element_type=F32,
            )
            result = part if result is None else result + part
        yield slice(i * width, (i + 1) * width), result


def expert_sent(first, second, ffn_gain, gate, up, down, dense_other):
    count = len(first)
    rows = first[0].shape[0]
    experts, model, ffe = gate.shape
    half = model // CORES
    tp_count = lax.axis_size("tp")
    width = model // tp_count
    z_count = tp_count // CORES
    total = experts * lax.axis_size("ep")

    def body(*refs):
        mine_refs, other_refs, refs = refs[:count], refs[count : 2 * count], refs[2 * count :]
        gain_ref, gate_ref, up_ref, down_ref, dense_ref, hidden_out, other_out = refs
        core = lax.axis_index("tp") % CORES
        start = lax.axis_index("ep") * experts
        mine = jnp.concatenate([r[:, :half].astype(F32) for r in mine_refs], 0)
        other = jnp.concatenate([r[:, :half].astype(F32) for r in other_refs], 0)
        values = interleave(mine, other, core, width)
        normed = (values * row_scale(values) * gain_ref[...]).astype(BF16)
        table = jnp.concatenate([r[:, half:].astype(F32) for r in mine_refs], 0)
        lane = lax.broadcasted_iota(jnp.int32, table.shape, 1)
        for j in range(experts):
            gated = jnp.dot(normed, gate_ref[j], preferred_element_type=F32)
            raised = jnp.dot(normed, up_ref[j], preferred_element_type=F32)
            picked = (lane == start + j) | (lane == start + j + total)
            share = jnp.sum(jnp.where(picked, table, 0.0), axis=-1, keepdims=True)
            hidden_out[:, j * ffe : (j + 1) * ffe] = (silu(gated) * raised * share).astype(BF16)
        for cols, part in down_blocks(hidden_out, down_ref, width, z_count, False):
            other_out[:rows, cols] = (part[:rows] + dense_ref[:, cols]).astype(BF16)
            other_out[rows:, cols] = part[rows:].astype(BF16)

    every = rows * count
    outs = [
        jax.ShapeDtypeStruct((every, experts * ffe), BF16),
        jax.ShapeDtypeStruct((every, half), BF16),
    ]
    operands = (*first, *second, ffn_gain, gate, up, down, dense_other)
    return local_kernel(body, outs, operands, 5 * every * model * ffe * experts)


def expert_kept(hidden, down, dense_mine):
    every = hidden.shape[0]
    rows, half = dense_mine.shape
    tp_count = lax.axis_size("tp")
    width = half * CORES // tp_count
    z_count = tp_count // CORES

    def body(hidden_ref, down_ref, dense_ref, out):
        for cols, part in down_blocks(hidden_ref, down_ref, width, z_count, True):
            out[:rows, cols] = part[:rows] + dense_ref[:, cols]
            out[rows:, cols] = part[rows:]

    outs = [jax.ShapeDtypeStruct((every, half), F32)]
    flops = 2 * every * half * hidden.shape[1]
    return local_kernel(body, outs, (hidden, down, dense_mine), flops)[0]


def layer(
    residual,
    mixer_gain,
    gate_proj,
    input_proj,
    write_proj,
    read_proj,
    step_proj,
    conv_weight,
    step_bias,
    log_rate,
    skip_gain,
    group_gain,
    ssm_state,
    conv_state,
    out_proj,
    ffn_gain,
    routes,
    route_weight,
    expert_gate,
    expert_up,
    expert_down,
    dense_gate,
    dense_up,
    dense_down,
    blend_weight,
):
    rows = residual.shape[0]
    depth, width = gate_proj.shape
    heads = ssm_state.shape[1]
    ep_count, tp_count = lax.axis_size("ep"), lax.axis_size("tp")
    z_count = tp_count // CORES
    tp_rank = lax.axis_index("tp")
    z_rank = tp_rank // CORES
    ep_rank = lax.axis_index("ep")
    ep_steps, z_steps = range(1, ep_count), range(1, z_count)
    sizes = ep_count, tp_count
    expert_total = expert_gate.shape[0] * ep_count
    as_row = lambda vector: vector.reshape(1, -1)

    slices = [
        lax.dynamic_slice_in_dim(residual, partner(ep_count, ep_rank, k) * depth, depth, 1)
        for k in ep_steps
    ]
    blocks = [send_ep(s, *sizes, k, cross=True) for k, s in zip(ep_steps, slices)]
    conv_rows = conv_state.transpose(1, 2, 0, 3)
    (
        scale, step, decay, skip, resid_half, conv_old, conv_last, gain, own, depth_gain, table, *weights
    ) = head_terms(
        residual, as_row(mixer_gain), step_proj.T, as_row(step_bias), as_row(log_rate),
        as_row(skip_gain), conv_rows, routes.T, route_weight.T, conv_weight.transpose(1, 0, 2),
        as_row(group_gain), (gate_proj, input_proj, write_proj, read_proj), heads, width, expert_total,
    )
    partials = project((own, *blocks), depth_gain, weights)
    parts = [partials[0]] + [send_ep(partials[k], *sizes, k, back=True) for k in ep_steps]
    state, out_weight = load((ssm_state, out_proj))
    projected, fed, written, mine, other = mix(
        parts, scale, step, decay, skip, conv_old, conv_last, state, gain, out_weight
    )

    mine = mine + send_core(other, tp_count).astype(F32)
    shared = mine.astype(BF16)
    gathered = [send_z(shared, *sizes, k) for k in z_steps]
    new_state, new_conv = advance_state(state, decay, fed, written, projected, conv_rows)
    new_conv = new_conv.transpose(2, 0, 1, 3)
    for part in gathered:
        mine = mine + part.astype(F32)
    resid_mid = (resid_half.astype(F32) + mine).astype(BF16)
    packed = jnp.concatenate((resid_mid, table), 1)

    seconds = [send_ep(packed, *sizes, k, cross=True) for k in ep_steps]
    own_other = send_core(packed, tp_count)
    dense_mine, dense_other = dense_branch(
        packed, own_other, as_row(ffn_gain), dense_gate, dense_up, dense_down, as_row(blend_weight)
    )
    firsts = [send_core(second, tp_count) for second in seconds]
    hidden, other = expert_sent(
        (packed, *firsts), (own_other, *seconds), as_row(ffn_gain), expert_gate, expert_up, expert_down,
        dense_other,
    )
    summed = send_core(other, tp_count)
    mine = expert_kept(hidden, expert_down, dense_mine) + summed.astype(F32)
    total = mine[:rows]
    low = mine.astype(BF16)
    for k in ep_steps:
        piece = low[k * rows : (k + 1) * rows]
        total = total + send_ep(piece, *sizes, k, back=True).astype(F32)
    low = total.astype(BF16)
    result = lax.dynamic_slice_in_dim(resid_mid, z_rank * width, width, 1).astype(F32)
    result = result + total[:, :width]
    for k in z_steps:
        piece = low[:, k * width : (k + 1) * width]
        result = result + send_z(piece, *sizes, k, cross=True).astype(F32)
    return result.astype(BF16), new_state, new_conv


def solution(mesh):
    return jax.shard_map(
        layer,
        mesh=mesh,
        in_specs=(
            P("ep", None),
            P(),
            P("ep", "tp"),
            P("ep", "tp"),
            P("ep", "tp"),
            P("ep", "tp"),
            P(),
            P(),
            P(),
            P(),
            P(),
            P(),
            P("ep", "tp", None, None),
            P("ep", None, None, "tp"),
            P("tp", None),
            P(),
            P("ep", None),
            P("ep", None),
            P("ep", None, "tp"),
            P("ep", None, "tp"),
            P("ep", "tp", None),
            P(None, "tp"),
            P(None, "tp"),
            P("tp", None),
            P(),
        ),
        out_specs=(P("ep", "tp"), P("ep", "tp", None, None), P("ep", None, None, "tp")),
        check_vma=False,
    )
```

```python
import jax
import jax.numpy as jnp
from jax import lax
from jax.experimental import pallas as pl
from jax.experimental.pallas import tpu as pltpu
from jax.sharding import PartitionSpec as P


epsilon = 1e-06
CORES = 2
LANES = 128
F32 = jnp.float32
BF16 = jnp.bfloat16
EXACT = lax.Precision.HIGHEST


def partner(count, index, step):
    return index ^ step if count & (count - 1) == 0 else (index + step) % count


def hop(block, pairs):
    return lax.ppermute(block, ("ep", "tp"), pairs)


def send_ep(block, ep_count, tp_count, step, cross=False, back=False):
    pairs = [
        (i * tp_count + t, partner(ep_count, i, step) * tp_count + (t ^ cross))
        for i in range(ep_count)
        for t in range(tp_count)
    ]
    return hop(block, [(b, a) for a, b in pairs] if back else pairs)


def send_z(block, ep_count, tp_count, step, cross=False):
    z_count = tp_count // CORES
    pairs = [
        (i * tp_count + z * CORES + c, i * tp_count + partner(z_count, z, step) * CORES + (c ^ cross))
        for i in range(ep_count)
        for z in range(z_count)
        for c in range(CORES)
    ]
    return hop(block, pairs)


def send_core(block, count):
    return lax.ppermute(block, "tp", [(i, i ^ 1) for i in range(count)])


def local_kernel(body, outs, operands, flops=0, scratch=(), remote=(), far_outs=()):
    near, far = pl.BlockSpec(memory_space=pltpu.VMEM), pl.BlockSpec(memory_space=pltpu.HBM)
    call = pl.pallas_call(
        body,
        out_shape=outs,
        in_specs=[far if i in remote else near for i in range(len(operands))],
        out_specs=[far if i in far_outs else near for i in range(len(outs))],
        scratch_shapes=scratch,
        cost_estimate=pl.CostEstimate(flops=flops, bytes_accessed=0, transcendentals=0),
        compiler_params=pltpu.CompilerParams(vmem_limit_bytes=40 << 20),
    )
    return call(
        *(
            pltpu.with_memory_space_constraint(x, pltpu.HBM) if i in remote else x
            for i, x in enumerate(operands)
        )
    )


def fetch(pairs, sems):
    copies = [pltpu.make_async_copy(a, b, sems.at[i]) for i, (a, b) in enumerate(pairs)]
    for copy in copies:
        copy.start()
    return copies


def row_scale(values):
    return lax.rsqrt(jnp.mean(values * values, axis=-1, keepdims=True) + epsilon)


def halves(array, core, width):
    count = array.shape[1] // width
    even = jnp.concatenate([array[:, i * width : (i + 1) * width] for i in range(0, count, 2)], 1)
    odd = jnp.concatenate([array[:, i * width : (i + 1) * width] for i in range(1, count, 2)], 1)
    first = core == 0
    return jnp.where(first, even, odd), jnp.where(first, odd, even)


def interleave(joined, mine, other, core, width):
    for array, parity in ((mine, core), (other, 1 - core)):
        top = 0
        for ref in array:
            rows = ref.shape[0]
            for i in range(joined.shape[1] // width // CORES):
                start = pl.multiple_of((i * CORES + parity) * width, LANES)
                joined[top : top + rows, pl.ds(start, width)] = ref[:, i * width : (i + 1) * width]
            top += rows


def project(blocks, gain, weights):
    rows = blocks[0].shape[0]
    depth, width = weights[0].shape
    count, kinds = len(blocks), len(weights)

    def body(*refs):
        ins, gain_ref, refs = refs[:count], refs[count], refs[count + 1 :]
        mats, outs = refs[:kinds], refs[kinds:]
        scaled = [(r[...].astype(F32) * gain_ref[...]).astype(BF16) for r in ins]
        stacked = jnp.concatenate(scaled, 0)
        for j, mat in enumerate(mats):
            result = jnp.dot(stacked, mat[...], preferred_element_type=F32)
            for i, out in enumerate(outs):
                piece = result[i * rows : (i + 1) * rows]
                out[:, j * width : (j + 1) * width] = piece.astype(out.dtype)

    outs = [jax.ShapeDtypeStruct((rows, kinds * width), BF16 if i else F32) for i in range(count)]
    flops = 2 * rows * count * depth * kinds * width
    return local_kernel(body, outs, (*blocks, gain, *weights), flops)


def head_terms(
    residual, mixer_gain, step_proj, step_bias, log_rate, skip_gain, conv_state, routes, route_weight,
    conv_weight, group_gain, weights, heads, width, expert_total,
):
    rows, model = residual.shape
    total = step_proj.shape[0]
    state = LANES
    kinds, taps = conv_weight.shape[:2]
    count = len(weights)
    depth = weights[0].shape[0]
    side = -(-2 * expert_total // LANES) * LANES
    fetched = (
        residual, mixer_gain, step_proj, step_bias, log_rate, skip_gain, routes, route_weight,
    )

    def body(*refs):
        sources, refs = refs[: len(fetched)], refs[len(fetched) :]
        conv_hbm, tap_hbm, group_hbm, refs = refs[0], refs[1], refs[2], refs[3:]
        weight_hbm, refs = refs[:count], refs[count:]
        (scale, step, decay, skip, half, old, last, gain_out), refs = refs[:8], refs[8:]
        (own_out, depth_gain, table_out, conv_ref), refs = refs[:4], refs[4:]
        weight_outs, refs = refs[:count], refs[count:]
        held, (tap_ref, sems) = refs[: len(fetched)], refs[len(fetched) :]
        res_ref, gain_ref, proj_ref, bias_ref, rate_ref, skip_ref, routes_ref, share_ref = held
        rank = lax.axis_index("tp")
        mine = pl.ds(pl.multiple_of(rank * width, LANES), width)
        copies = fetch(
            (
                *zip(sources, held),
                (conv_hbm, conv_ref),
                (tap_hbm.at[:, :, mine], tap_ref),
                (group_hbm.at[:, mine], gain_out),
                *zip(weight_hbm, weight_outs),
            ),
            sems,
        )
        local = len(fetched) + 3
        for copy in copies[:local]:
            copy.wait()
        head_start = rank * heads
        values = res_ref[...].astype(F32)
        scaling = row_scale(values)
        normed = (values * scaling * gain_ref[...]).astype(BF16)
        raw = lax.dot_general(
            normed, proj_ref[...], (((1,), (1,)), ((), ())), preferred_element_type=F32
        )
        raw = raw + bias_ref[...]
        size = jnp.maximum(raw, 0.0) + jnp.log1p(jnp.exp(-jnp.abs(raw)))
        fade = jnp.exp(-jnp.exp(rate_ref[...]) * size)

        def spread(table, lanes):
            head = lax.broadcasted_iota(jnp.int32, (total, heads * lanes), 0) - head_start
            lane = lax.broadcasted_iota(jnp.int32, (total, heads * lanes), 1)
            hot = ((lane >= head * lanes) & (lane < (head + 1) * lanes)).astype(F32)
            return jnp.dot(table, hot, preferred_element_type=F32, precision=EXACT)

        scale[...] = jnp.broadcast_to(scaling, (rows, LANES))
        step[...] = spread(size, width // heads)
        decay[...] = spread(fade, state)
        skip[...] = spread(jnp.broadcast_to(skip_ref[...], (8, total)), width // heads)
        half[...] = halves(values, rank % CORES, width)[0].astype(BF16)
        for j in range(kinds):
            part = conv_ref[0, j].astype(F32) * tap_ref[j, 0:1]
            for k in range(1, taps - 1):
                part = part + conv_ref[k, j].astype(F32) * tap_ref[j, k : k + 1]
            old[j] = part
            last[j : j + 1, :] = tap_ref[j, taps - 1 : taps]
        owned = pl.ds(pl.multiple_of(lax.axis_index("ep") * depth, LANES), depth)
        own_out[...] = res_ref[:, owned]
        depth_gain[...] = gain_ref[:, owned]
        slot = lax.broadcasted_iota(jnp.int32, (side, rows), 0)
        named = jnp.where(slot < expert_total, slot, slot - expert_total)
        table = jnp.zeros((side, rows), F32)
        for k in range(routes.shape[0]):
            table = table + jnp.where(
                routes_ref[k : k + 1, :] == named, share_ref[k : k + 1, :], 0.0
            )
        high = table.astype(BF16).astype(F32)
        table_out[...] = jnp.where(slot < expert_total, high, table - high).T.astype(BF16)
        for copy in copies[local:]:
            copy.wait()

    outs = [
        jax.ShapeDtypeStruct((rows, LANES), F32),
        jax.ShapeDtypeStruct((rows, width), F32),
        jax.ShapeDtypeStruct((rows, heads * state), F32),
        jax.ShapeDtypeStruct((8, width), F32),
        jax.ShapeDtypeStruct((rows, model // CORES), BF16),
        jax.ShapeDtypeStruct((kinds, rows, width), F32),
        jax.ShapeDtypeStruct((8, width), F32),
        jax.ShapeDtypeStruct((1, width), F32),
        jax.ShapeDtypeStruct((rows, depth), BF16),
        jax.ShapeDtypeStruct((1, depth), F32),
        jax.ShapeDtypeStruct((rows, side), BF16),
        jax.ShapeDtypeStruct(conv_state.shape, conv_state.dtype),
        *(jax.ShapeDtypeStruct(w.shape, w.dtype) for w in weights),
    ]
    operands = (*fetched, conv_state, conv_weight, group_gain, *weights)
    scratch = [
        *(pltpu.VMEM(x.shape, x.dtype) for x in fetched),
        pltpu.VMEM((kinds, taps, width), F32),
        pltpu.SemaphoreType.DMA((len(operands),)),
    ]
    flops = 2 * rows * model * total
    return local_kernel(body, outs, operands, flops, scratch, range(len(operands)))


def load_state(ssm_state, out_proj):
    rows, heads, head_dim, state = ssm_state.shape
    width = heads * head_dim
    chunk = 8
    pieces = rows // chunk

    def body(state_hbm, proj_hbm, state_out, low_out, proj_out, sems):
        spans = [pl.ds(i * chunk, chunk) for i in range(pieces)]
        copies = fetch(
            [(state_hbm.at[s], state_out.at[s]) for s in spans] + [(proj_hbm, proj_out)], sems
        )
        for copy, span in zip(copies, spans):
            copy.wait()
            low = state_out[span].reshape(chunk // 2, 2, width, state).astype(BF16)
            pair = pl.ds(span.start // 2, chunk // 2)
            low_out[pair, :, :state] = low[:, 0]
            low_out[pair, :, state:] = low[:, 1]
        copies[-1].wait()

    outs = [
        jax.ShapeDtypeStruct(ssm_state.shape, F32),
        jax.ShapeDtypeStruct((rows // 2, width, 2 * state), BF16),
        jax.ShapeDtypeStruct(out_proj.shape, out_proj.dtype),
    ]
    scratch = [pltpu.SemaphoreType.DMA((pieces + 1,))]
    return local_kernel(body, outs, (ssm_state, out_proj), 0, scratch, range(2))


def silu(values):
    return values * jax.nn.sigmoid(values)


def mix(partials, scale, step, decay, skip, conv_old, conv_last, ssm_state, group_gain, out_proj):
    width, state = ssm_state.shape[1], ssm_state.shape[2] // 2
    rows = ssm_state.shape[0] * 2
    heads = decay.shape[1] // state
    head_dim = width // heads
    model = out_proj.shape[1]
    groups = width // state
    count = len(partials)

    def body(*refs):
        parts = refs[:count]
        (scale_ref, step_ref, decay_ref, skip_ref, old_ref, last_ref, state_ref, gain_ref, out_ref) = refs[
            count : count + 9
        ]
        proj_out, fed_out, write_out, mine_out, other_out, read_buf, sum_buf = refs[count + 9 :]
        rank = lax.axis_index("tp")
        summed = parts[0][...].astype(F32)
        for part in parts[1:]:
            summed = summed + part[...].astype(F32)
        projected = (summed * scale_ref[:, :1]).astype(BF16)
        proj_out[...] = projected
        fresh = projected.astype(F32)
        act = [
            silu(old_ref[j] + fresh[:, (j + 1) * width : (j + 2) * width] * last_ref[j : j + 1, :])
            for j in range(3)
        ]
        x_act, b_act, c_act = act
        fed = step_ref[...] * x_act
        fed_out[...] = fed
        write_out[...] = b_act
        c_low = c_act.astype(BF16)
        read_buf[...] = c_low.astype(F32)
        lane = lax.broadcasted_iota(jnp.int32, (1, width), 1)
        empty = jnp.zeros((1, state), F32)
        for s in range(0, rows, 2):
            reads = []
            for t in range(2):
                for g in range(groups):
                    read = read_buf[s + t : s + t + 1, g * state : (g + 1) * state]
                    reads.append(jnp.concatenate([empty, read] if t else [read, empty], 1))
            reads.append(jnp.zeros((8 - 2 * groups, 2 * state), F32))
            found = lax.dot_general(
                jnp.concatenate(reads, 0).astype(BF16),
                state_ref[s // 2],
                (((1,), (1,)), ((), ())),
                preferred_element_type=F32,
            )
            for t in range(2):
                row = found[t * groups : t * groups + 1]
                for g in range(1, groups):
                    row = jnp.where(lane >= g * state, found[t * groups + g : t * groups + g + 1], row)
                sum_buf[s + t : s + t + 1, :] = row
        old_part = sum_buf[...]
        decay_ch = jnp.concatenate(
            [decay_ref[:, h * state : h * state + head_dim] for h in range(heads)], 1
        )
        both = []
        for g in range(groups):
            cols = slice(g * state, (g + 1) * state)
            inner = jnp.sum(b_act[:, cols] * c_act[:, cols], axis=-1, keepdims=True)
            both.append(fed[:, cols] * inner)
        ssm_out = decay_ch * old_part + jnp.concatenate(both, 1) + skip_ref[0:1] * x_act
        gated = ssm_out * silu(fresh[:, :width])
        gain = gain_ref[...]
        mixed = []
        for g in range(groups):
            cols = slice(g * state, (g + 1) * state)
            mixed.append(gated[:, cols] * row_scale(gated[:, cols]) * gain[:, cols])
        mixed = jnp.concatenate(mixed, 1).astype(BF16)
        core = rank % CORES
        for out, parity in ((other_out, 1 - core), (mine_out, core)):
            for i in range(model // width // CORES):
                start = pl.multiple_of((i * CORES + parity) * width, LANES)
                part = jnp.dot(mixed, out_ref[:, pl.ds(start, width)], preferred_element_type=F32)
                out[:, i * width : (i + 1) * width] = part.astype(out.dtype)

    outs = [
        jax.ShapeDtypeStruct((rows, partials[0].shape[1]), BF16),
        jax.ShapeDtypeStruct((rows, width), F32),
        jax.ShapeDtypeStruct((rows, width), F32),
        jax.ShapeDtypeStruct((rows, model // CORES), F32),
        jax.ShapeDtypeStruct((rows, model // CORES), BF16),
    ]
    operands = (
        *partials, scale, step, decay, skip, conv_old, conv_last, ssm_state, group_gain, out_proj,
    )
    scratch = [pltpu.VMEM((rows, width), F32), pltpu.VMEM((rows, width), F32)]
    return local_kernel(body, outs, operands, 2 * rows * width * model, scratch)


def advance_state(ssm_state, decay, fed, written, projected, conv_state):
    rows, heads, head_dim, state = ssm_state.shape
    width = heads * head_dim
    groups = width // state
    per_group = heads // groups
    taps, kinds = conv_state.shape[:2]
    chunk = 8

    def body(state_ref, decay_ref, fed_ref, write_ref, proj_ref, conv_ref, out_hbm, conv_out, *scratch):
        buf, fresh, sems = scratch
        shift = pltpu.make_async_copy(
            conv_ref.at[1:], conv_out.at[: taps - 1], sems.at[rows // chunk]
        )
        shift.start()
        for j in range(kinds):
            fresh[j] = proj_ref[:, (j + 1) * width : (j + 2) * width]
        newest = pltpu.make_async_copy(fresh, conv_out.at[taps - 1], sems.at[rows // chunk + 1])
        newest.start()
        fed_cols = fed_ref[...].T
        copies = [shift, newest]
        for s in range(rows):
            for h in range(heads):
                g = h // per_group
                fade = decay_ref[s : s + 1, h * state : (h + 1) * state]
                write = write_ref[s : s + 1, g * state : (g + 1) * state]
                column = fed_cols[h * head_dim : (h + 1) * head_dim, s : s + 1]
                buf[s, h] = fade * state_ref[s, h] + column * write
            if s % chunk == chunk - 1:
                span = pl.ds(s - chunk + 1, chunk)
                done = pltpu.make_async_copy(buf.at[span], out_hbm.at[span], sems.at[s // chunk])
                done.start()
                copies.append(done)
        for copy in copies:
            copy.wait()

    outs = [
        jax.ShapeDtypeStruct(ssm_state.shape, F32),
        jax.ShapeDtypeStruct(conv_state.shape, conv_state.dtype),
    ]
    scratch = [
        pltpu.VMEM(ssm_state.shape, F32),
        pltpu.VMEM((kinds, rows, width), conv_state.dtype),
        pltpu.SemaphoreType.DMA((rows // chunk + 2,)),
    ]
    operands = (ssm_state, decay, fed, written, projected, conv_state)
    return local_kernel(body, outs, operands, 8 << 20, scratch, (), (0, 1))


def column_blocks(width, z_count, kept):
    rank = lax.axis_index("tp")
    z, core = rank // CORES, rank % CORES
    starts = []
    for step in range(z_count):
        same = (step == 0) == kept
        parity = core if same else 1 - core
        starts.append(pl.multiple_of((partner(z_count, z, step) * CORES + parity) * width, LANES))
    return starts


def dense_branch(mine, other, ffn_gain, gate, up, down, blend):
    rows = mine.shape[0]
    model = gate.shape[0]
    half = model // CORES
    tp_count = lax.axis_size("tp")
    width = model // tp_count
    z_count = tp_count // CORES

    def body(
        mine_ref, other_ref, gain_ref, gate_ref, up_ref, down_ref, blend_ref, mine_out, other_out, joined
    ):
        interleave(joined, [mine_ref], [other_ref], lax.axis_index("tp") % CORES, width)
        values = joined[...].astype(F32)
        normed = (values * row_scale(values) * gain_ref[...]).astype(BF16)
        gated = jnp.dot(normed, gate_ref[...], preferred_element_type=F32)
        raised = jnp.dot(normed, up_ref[...], preferred_element_type=F32)
        hidden = (silu(gated) * raised).astype(BF16)
        weight = jax.nn.sigmoid(
            jnp.sum(normed.astype(F32) * blend_ref[...].astype(F32), axis=-1, keepdims=True)
        )
        for kept, out in ((True, mine_out), (False, other_out)):
            for i, start in enumerate(column_blocks(width, z_count, kept)):
                part = jnp.dot(hidden, down_ref[:, pl.ds(start, width)], preferred_element_type=F32)
                out[:, i * width : (i + 1) * width] = part * weight

    outs = [jax.ShapeDtypeStruct((rows, half), F32)] * 2
    operands = (mine, other, ffn_gain, gate, up, down, blend)
    flops = 6 * rows * model * gate.shape[1]
    scratch = [pltpu.VMEM((rows, model), BF16)]
    return local_kernel(body, outs, operands, flops, scratch)


def down_blocks(hidden, down_ref, width, z_count, kept):
    ffe = down_ref.shape[1]
    for i, start in enumerate(column_blocks(width, z_count, kept)):
        result = None
        for j in range(down_ref.shape[0]):
            part = jnp.dot(
                hidden[:, j * ffe : (j + 1) * ffe],
                down_ref[j, :, pl.ds(start, width)],
                preferred_element_type=F32,
            )
            result = part if result is None else result + part
        yield slice(i * width, (i + 1) * width), result


def half_rows(width, core_parity, blocks):
    return [pl.multiple_of((i * CORES + core_parity) * width, LANES) for i in range(blocks)]


def half_product(refs, gain_ref, mats, starts, width):
    half = width * len(starts)
    values = jnp.concatenate([r[:, :half] for r in refs], 0).astype(F32)
    gain = jnp.concatenate([gain_ref[:, pl.ds(s, width)] for s in starts], 1)
    scaled = (values * gain).astype(BF16)
    products = []
    for ref, j in mats:
        weights = jnp.concatenate([ref[j, pl.ds(s, width), :] for s in starts], 0)
        products.append(jnp.dot(scaled, weights, preferred_element_type=F32))
    return products, jnp.sum(values * values, axis=-1, keepdims=True)


def expert_first(first, ffn_gain, gate, up, down):
    count = len(first)
    every = first[0].shape[0] * count
    experts, model, ffe = gate.shape
    tp_count = lax.axis_size("tp")
    width = model // tp_count

    def body(*refs):
        gain_ref, gate_ref, up_ref, _, partial_out, square_out = refs[count:]
        starts = half_rows(width, lax.axis_index("tp") % CORES, tp_count // CORES)
        mats = [(ref, j) for j in range(experts) for ref in (gate_ref, up_ref)]
        products, squares = half_product(refs[:count], gain_ref, mats, starts, width)
        for i, product in enumerate(products):
            partial_out[:, i * ffe : (i + 1) * ffe] = product
        square_out[...] = jnp.broadcast_to(squares, square_out.shape)

    outs = [
        jax.ShapeDtypeStruct((every, 2 * experts * ffe), F32),
        jax.ShapeDtypeStruct((every, LANES), F32),
    ]
    flops = 2 * every * model * ffe * experts
    return local_kernel(body, outs, (*first, ffn_gain, gate, up, down), flops)


def expert_sent(partial, squares, tables, second, ffn_gain, gate, up, down, dense_other):
    count = len(second)
    rows = second[0].shape[0]
    experts, model, ffe = gate.shape
    half = model // CORES
    tp_count = lax.axis_size("tp")
    width = model // tp_count
    z_count = tp_count // CORES
    total = experts * lax.axis_size("ep")

    def body(partial_ref, square_ref, *refs):
        table_refs, other_refs, refs = refs[:count], refs[count : 2 * count], refs[2 * count :]
        gain_ref, gate_ref, up_ref, down_ref, dense_ref, hidden_out, other_out = refs
        starts = half_rows(width, 1 - lax.axis_index("tp") % CORES, z_count)
        mats = [(ref, j) for j in range(experts) for ref in (gate_ref, up_ref)]
        products, others = half_product(other_refs, gain_ref, mats, starts, width)
        scale = lax.rsqrt((square_ref[:, :1] + others) / model + epsilon)
        products = [
            (p + partial_ref[:, i * ffe : (i + 1) * ffe]) * scale for i, p in enumerate(products)
        ]
        start = lax.axis_index("ep") * experts
        table = jnp.concatenate([r[:, half:].astype(F32) for r in table_refs], 0)
        lane = lax.broadcasted_iota(jnp.int32, table.shape, 1)
        for j in range(experts):
            gated, raised = products[2 * j], products[2 * j + 1]
            picked = (lane == start + j) | (lane == start + j + total)
            share = jnp.sum(jnp.where(picked, table, 0.0), axis=-1, keepdims=True)
            hidden_out[:, j * ffe : (j + 1) * ffe] = (silu(gated) * raised * share).astype(BF16)
        for cols, part in down_blocks(hidden_out, down_ref, width, z_count, False):
            other_out[:rows, cols] = (part[:rows] + dense_ref[:, cols]).astype(BF16)
            other_out[rows:, cols] = part[rows:].astype(BF16)

    every = rows * count
    outs = [
        jax.ShapeDtypeStruct((every, experts * ffe), BF16),
        jax.ShapeDtypeStruct((every, half), BF16),
    ]
    operands = (partial, squares, *tables, *second, ffn_gain, gate, up, down, dense_other)
    return local_kernel(body, outs, operands, 3 * every * model * ffe * experts)


def expert_kept(hidden, down, dense_mine):
    every = hidden.shape[0]
    rows, half = dense_mine.shape
    tp_count = lax.axis_size("tp")
    width = half * CORES // tp_count
    z_count = tp_count // CORES

    def body(hidden_ref, down_ref, dense_ref, out):
        for cols, part in down_blocks(hidden_ref, down_ref, width, z_count, True):
            out[:rows, cols] = part[:rows] + dense_ref[:, cols]
            out[rows:, cols] = part[rows:]

    outs = [jax.ShapeDtypeStruct((every, half), F32)]
    flops = 2 * every * half * hidden.shape[1]
    return local_kernel(body, outs, (hidden, down, dense_mine), flops)[0]


def layer(
    residual,
    mixer_gain,
    gate_proj,
    input_proj,
    write_proj,
    read_proj,
    step_proj,
    conv_weight,
    step_bias,
    log_rate,
    skip_gain,
    group_gain,
    ssm_state,
    conv_state,
    out_proj,
    ffn_gain,
    routes,
    route_weight,
    expert_gate,
    expert_up,
    expert_down,
    dense_gate,
    dense_up,
    dense_down,
    blend_weight,
):
    rows = residual.shape[0]
    depth, width = gate_proj.shape
    heads = ssm_state.shape[1]
    ep_count, tp_count = lax.axis_size("ep"), lax.axis_size("tp")
    z_count = tp_count // CORES
    tp_rank = lax.axis_index("tp")
    z_rank = tp_rank // CORES
    ep_rank = lax.axis_index("ep")
    ep_steps, z_steps = range(1, ep_count), range(1, z_count)
    sizes = ep_count, tp_count
    expert_total = expert_gate.shape[0] * ep_count
    as_row = lambda vector: vector.reshape(1, -1)

    slices = [
        lax.dynamic_slice_in_dim(residual, partner(ep_count, ep_rank, k) * depth, depth, 1)
        for k in ep_steps
    ]
    blocks = [send_ep(s, *sizes, k, cross=True) for k, s in zip(ep_steps, slices)]
    conv_rows = conv_state.transpose(1, 2, 0, 3)
    (
        scale, step, decay, skip, resid_half, conv_old, conv_last, gain, own, depth_gain, table, conv_held,
        *weights,
    ) = head_terms(
        residual, as_row(mixer_gain), step_proj.T, as_row(step_bias), as_row(log_rate),
        as_row(skip_gain), conv_rows, routes.T, route_weight.T, conv_weight.transpose(1, 0, 2),
        as_row(group_gain), (gate_proj, input_proj, write_proj, read_proj), heads, width, expert_total,
    )
    partials = project((own, *blocks), depth_gain, weights)
    parts = [partials[0]] + [send_ep(partials[k], *sizes, k, back=True) for k in ep_steps]
    state, low_state, out_weight = load_state(ssm_state, out_proj)
    projected, fed, written, mine, other = mix(
        parts, scale, step, decay, skip, conv_old, conv_last, low_state, gain, out_weight
    )

    mine = mine + send_core(other, tp_count).astype(F32)
    shared = mine.astype(BF16)
    gathered = [send_z(shared, *sizes, k) for k in z_steps]
    new_state, new_conv = advance_state(state, decay, fed, written, projected, conv_held)
    new_conv = new_conv.transpose(2, 0, 1, 3)
    for part in gathered:
        mine = mine + part.astype(F32)
    resid_mid = (resid_half.astype(F32) + mine).astype(BF16)
    packed = jnp.concatenate((resid_mid, table), 1)

    seconds = [send_ep(packed, *sizes, k) for k in ep_steps]
    own_other = send_core(packed, tp_count)
    dense_mine, dense_other = dense_branch(
        packed, own_other, as_row(ffn_gain), dense_gate, dense_up, dense_down, as_row(blend_weight)
    )
    firsts = []
    for k, second in zip(ep_steps, seconds):
        cut = second[:, : resid_mid.shape[1]]
        firsts.append(send_core(cut, tp_count))
    tokens = (packed, *seconds)
    partial, squares = expert_first(tokens, as_row(ffn_gain), expert_gate, expert_up, expert_down)
    hidden, other = expert_sent(
        partial, squares, tokens, (own_other, *firsts), as_row(ffn_gain), expert_gate, expert_up,
        expert_down, dense_other,
    )
    summed = send_core(other, tp_count)
    mine = expert_kept(hidden, expert_down, dense_mine) + summed.astype(F32)
    total = mine[:rows]
    low = mine.astype(BF16)
    for k in ep_steps:
        piece = low[k * rows : (k + 1) * rows]
        total = total + send_ep(piece, *sizes, k, back=True).astype(F32)
    low = total.astype(BF16)
    result = lax.dynamic_slice_in_dim(resid_mid, z_rank * width, width, 1).astype(F32)
    result = result + total[:, :width]
    for k in z_steps:
        piece = low[:, k * width : (k + 1) * width]
        result = result + send_z(piece, *sizes, k, cross=True).astype(F32)
    return result.astype(BF16), new_state, new_conv


def solution(mesh):
    return jax.shard_map(
        layer,
        mesh=mesh,
        in_specs=(
            P("ep", None),
            P(),
            P("ep", "tp"),
            P("ep", "tp"),
            P("ep", "tp"),
            P("ep", "tp"),
            P(),
            P(),
            P(),
            P(),
            P(),
            P(),
            P("ep", "tp", None, None),
            P("ep", None, None, "tp"),
            P("tp", None),
            P(),
            P("ep", None),
            P("ep", None),
            P("ep", None, "tp"),
            P("ep", None, "tp"),
            P("ep", "tp", None),
            P(None, "tp"),
            P(None, "tp"),
            P("tp", None),
            P(),
        ),
        out_specs=(P("ep", "tp"), P("ep", "tp", None, None), P("ep", None, None, "tp")),
        check_vma=False,
    )
```

```python
import jax
import jax.numpy as jnp
from jax import lax
from jax.experimental import pallas as pl
from jax.experimental.pallas import tpu as pltpu
from jax.sharding import PartitionSpec as P


epsilon = 1e-06
CORES = 2
LANES = 128
F32 = jnp.float32
BF16 = jnp.bfloat16
EXACT = lax.Precision.HIGHEST


def partner(count, index, step):
    return index ^ step if count & (count - 1) == 0 else (index + step) % count


def hop(block, pairs):
    return lax.ppermute(block, ("ep", "tp"), pairs)


def send_ep(block, ep_count, tp_count, step, cross=False, back=False):
    pairs = [
        (i * tp_count + t, partner(ep_count, i, step) * tp_count + (t ^ cross))
        for i in range(ep_count)
        for t in range(tp_count)
    ]
    return hop(block, [(b, a) for a, b in pairs] if back else pairs)


def send_z(block, ep_count, tp_count, step, cross=False):
    z_count = tp_count // CORES
    pairs = [
        (i * tp_count + z * CORES + c, i * tp_count + partner(z_count, z, step) * CORES + (c ^ cross))
        for i in range(ep_count)
        for z in range(z_count)
        for c in range(CORES)
    ]
    return hop(block, pairs)


def send_core(block, count):
    return lax.ppermute(block, "tp", [(i, i ^ 1) for i in range(count)])


def local_kernel(body, outs, operands, flops=0, scratch=(), remote=(), far_outs=()):
    near, far = pl.BlockSpec(memory_space=pltpu.VMEM), pl.BlockSpec(memory_space=pltpu.HBM)
    call = pl.pallas_call(
        body,
        out_shape=outs,
        in_specs=[far if i in remote else near for i in range(len(operands))],
        out_specs=[far if i in far_outs else near for i in range(len(outs))],
        scratch_shapes=scratch,
        cost_estimate=pl.CostEstimate(flops=flops, bytes_accessed=0, transcendentals=0),
        compiler_params=pltpu.CompilerParams(vmem_limit_bytes=40 << 20),
    )
    return call(
        *(
            pltpu.with_memory_space_constraint(x, pltpu.HBM) if i in remote else x
            for i, x in enumerate(operands)
        )
    )


def fetch(pairs, sems):
    copies = [pltpu.make_async_copy(a, b, sems.at[i]) for i, (a, b) in enumerate(pairs)]
    for copy in copies:
        copy.start()
    return copies


def row_scale(values):
    return lax.rsqrt(jnp.mean(values * values, axis=-1, keepdims=True) + epsilon)


def halves(array, core, width):
    count = array.shape[1] // width
    even = jnp.concatenate([array[:, i * width : (i + 1) * width] for i in range(0, count, 2)], 1)
    odd = jnp.concatenate([array[:, i * width : (i + 1) * width] for i in range(1, count, 2)], 1)
    first = core == 0
    return jnp.where(first, even, odd), jnp.where(first, odd, even)


def half_rows(width, core_parity, blocks):
    return [pl.multiple_of((i * CORES + core_parity) * width, LANES) for i in range(blocks)]


def interleave(joined, mine, other, core, width):
    for array, parity in ((mine, core), (other, 1 - core)):
        top = 0
        for ref in array:
            rows = ref.shape[0]
            for i in range(joined.shape[1] // width // CORES):
                start = pl.multiple_of((i * CORES + parity) * width, LANES)
                joined[top : top + rows, pl.ds(start, width)] = ref[:, i * width : (i + 1) * width]
            top += rows


def project(blocks, gain, weights):
    rows = blocks[0].shape[0]
    depth, width = weights[0].shape
    count, kinds = len(blocks), len(weights)

    def body(*refs):
        ins, gain_ref, refs = refs[:count], refs[count], refs[count + 1 :]
        mats, outs = refs[:kinds], refs[kinds:]
        scaled = [(r[...].astype(F32) * gain_ref[...]).astype(BF16) for r in ins]
        stacked = jnp.concatenate(scaled, 0)
        for j, mat in enumerate(mats):
            result = jnp.dot(stacked, mat[...], preferred_element_type=F32)
            for i, out in enumerate(outs):
                piece = result[i * rows : (i + 1) * rows]
                out[:, j * width : (j + 1) * width] = piece.astype(out.dtype)

    outs = [jax.ShapeDtypeStruct((rows, kinds * width), BF16 if i else F32) for i in range(count)]
    flops = 2 * rows * count * depth * kinds * width
    return local_kernel(body, outs, (*blocks, gain, *weights), flops)


def head_terms(
    residual, mixer_gain, step_proj, step_bias, log_rate, skip_gain, conv_state, routes, route_weight,
    conv_weight, group_gain, weights, heads, width, expert_total,
):
    rows, model = residual.shape
    total = step_proj.shape[0]
    state = LANES
    kinds, taps = conv_weight.shape[:2]
    count = len(weights)
    depth = weights[0].shape[0]
    side = -(-2 * expert_total // LANES) * LANES
    fetched = (
        residual, mixer_gain, step_proj, step_bias, log_rate, skip_gain, routes, route_weight,
    )

    def body(*refs):
        sources, refs = refs[: len(fetched)], refs[len(fetched) :]
        conv_hbm, tap_hbm, group_hbm, refs = refs[0], refs[1], refs[2], refs[3:]
        weight_hbm, refs = refs[:count], refs[count:]
        (scale, step, decay, skip, half, old, last, gain_out), refs = refs[:8], refs[8:]
        (own_out, depth_gain, table_out, conv_ref), refs = refs[:4], refs[4:]
        weight_outs, refs = refs[:count], refs[count:]
        held, (tap_ref, sems) = refs[: len(fetched)], refs[len(fetched) :]
        res_ref, gain_ref, proj_ref, bias_ref, rate_ref, skip_ref, routes_ref, share_ref = held
        rank = lax.axis_index("tp")
        mine = pl.ds(pl.multiple_of(rank * width, LANES), width)
        copies = fetch(
            (
                *zip(sources, held),
                (conv_hbm, conv_ref),
                (tap_hbm.at[:, :, mine], tap_ref),
                (group_hbm.at[:, mine], gain_out),
                *zip(weight_hbm, weight_outs),
            ),
            sems,
        )
        local = len(fetched) + 3
        for copy in copies[:local]:
            copy.wait()
        head_start = rank * heads
        values = res_ref[...].astype(F32)
        scaling = row_scale(values)
        normed = (values * scaling * gain_ref[...]).astype(BF16)
        raw = lax.dot_general(
            normed, proj_ref[...], (((1,), (1,)), ((), ())), preferred_element_type=F32
        )
        raw = raw + bias_ref[...]
        size = jnp.maximum(raw, 0.0) + jnp.log1p(jnp.exp(-jnp.abs(raw)))
        fade = jnp.exp(-jnp.exp(rate_ref[...]) * size)

        def spread(table, lanes):
            head = lax.broadcasted_iota(jnp.int32, (total, heads * lanes), 0) - head_start
            lane = lax.broadcasted_iota(jnp.int32, (total, heads * lanes), 1)
            hot = ((lane >= head * lanes) & (lane < (head + 1) * lanes)).astype(F32)
            return jnp.dot(table, hot, preferred_element_type=F32, precision=EXACT)

        scale[...] = jnp.broadcast_to(scaling, (rows, LANES))
        step[...] = spread(size, width // heads)
        decay[...] = spread(fade, state)
        skip[...] = spread(jnp.broadcast_to(skip_ref[...], (8, total)), width // heads)
        half[...] = halves(values, rank % CORES, width)[0].astype(BF16)
        for j in range(kinds):
            part = conv_ref[0, j].astype(F32) * tap_ref[j, 0:1]
            for k in range(1, taps - 1):
                part = part + conv_ref[k, j].astype(F32) * tap_ref[j, k : k + 1]
            old[j] = part
            last[j : j + 1, :] = tap_ref[j, taps - 1 : taps]
        owned = pl.ds(pl.multiple_of(lax.axis_index("ep") * depth, LANES), depth)
        own_out[...] = res_ref[:, owned]
        depth_gain[...] = gain_ref[:, owned]
        slot = lax.broadcasted_iota(jnp.int32, (side, rows), 0)
        named = jnp.where(slot < expert_total, slot, slot - expert_total)
        table = jnp.zeros((side, rows), F32)
        for k in range(routes.shape[0]):
            table = table + jnp.where(
                routes_ref[k : k + 1, :] == named, share_ref[k : k + 1, :], 0.0
            )
        high = table.astype(BF16).astype(F32)
        table_out[...] = jnp.where(slot < expert_total, high, table - high).T.astype(BF16)
        for copy in copies[local:]:
            copy.wait()

    outs = [
        jax.ShapeDtypeStruct((rows, LANES), F32),
        jax.ShapeDtypeStruct((rows, width), F32),
        jax.ShapeDtypeStruct((rows, heads * state), F32),
        jax.ShapeDtypeStruct((8, width), F32),
        jax.ShapeDtypeStruct((rows, model // CORES), BF16),
        jax.ShapeDtypeStruct((kinds, rows, width), F32),
        jax.ShapeDtypeStruct((8, width), F32),
        jax.ShapeDtypeStruct((1, width), F32),
        jax.ShapeDtypeStruct((rows, depth), BF16),
        jax.ShapeDtypeStruct((1, depth), F32),
        jax.ShapeDtypeStruct((rows, side), BF16),
        jax.ShapeDtypeStruct(conv_state.shape, conv_state.dtype),
        *(jax.ShapeDtypeStruct(w.shape, w.dtype) for w in weights),
    ]
    operands = (*fetched, conv_state, conv_weight, group_gain, *weights)
    scratch = [
        *(pltpu.VMEM(x.shape, x.dtype) for x in fetched),
        pltpu.VMEM((kinds, taps, width), F32),
        pltpu.SemaphoreType.DMA((len(operands),)),
    ]
    flops = 2 * rows * model * total
    return local_kernel(body, outs, operands, flops, scratch, range(len(operands)))


def load_state(ssm_state, out_proj):
    rows, heads, head_dim, state = ssm_state.shape
    width = heads * head_dim
    chunk = 8
    pieces = rows // chunk

    def body(state_hbm, proj_hbm, state_out, low_out, proj_out, sems):
        spans = [pl.ds(i * chunk, chunk) for i in range(pieces)]
        copies = fetch(
            [(state_hbm.at[s], state_out.at[s]) for s in spans] + [(proj_hbm, proj_out)], sems
        )
        for copy, span in zip(copies, spans):
            copy.wait()
            low = state_out[span].reshape(chunk // 2, 2, width, state).astype(BF16)
            pair = pl.ds(span.start // 2, chunk // 2)
            low_out[pair, :, :state] = low[:, 0]
            low_out[pair, :, state:] = low[:, 1]
        copies[-1].wait()

    outs = [
        jax.ShapeDtypeStruct(ssm_state.shape, F32),
        jax.ShapeDtypeStruct((rows // 2, width, 2 * state), BF16),
        jax.ShapeDtypeStruct(out_proj.shape, out_proj.dtype),
    ]
    scratch = [pltpu.SemaphoreType.DMA((pieces + 1,))]
    return local_kernel(body, outs, (ssm_state, out_proj), 0, scratch, range(2))


def silu(values):
    return values * jax.nn.sigmoid(values)


def mix(partials, scale, step, decay, skip, conv_old, conv_last, ssm_state, group_gain, out_proj):
    width, state = ssm_state.shape[1], ssm_state.shape[2] // 2
    rows = ssm_state.shape[0] * 2
    heads = decay.shape[1] // state
    head_dim = width // heads
    model = out_proj.shape[1]
    groups = width // state
    count = len(partials)

    def body(*refs):
        parts = refs[:count]
        (scale_ref, step_ref, decay_ref, skip_ref, old_ref, last_ref, state_ref, gain_ref, out_ref) = refs[
            count : count + 9
        ]
        proj_out, fed_out, write_out, mixed_out, other_out, read_buf, sum_buf = refs[count + 9 :]
        rank = lax.axis_index("tp")
        summed = parts[0][...].astype(F32)
        for part in parts[1:]:
            summed = summed + part[...].astype(F32)
        projected = (summed * scale_ref[:, :1]).astype(BF16)
        proj_out[...] = projected
        fresh = projected.astype(F32)
        act = [
            silu(old_ref[j] + fresh[:, (j + 1) * width : (j + 2) * width] * last_ref[j : j + 1, :])
            for j in range(3)
        ]
        x_act, b_act, c_act = act
        fed = step_ref[...] * x_act
        fed_out[...] = fed
        write_out[...] = b_act
        c_low = c_act.astype(BF16)
        read_buf[...] = c_low.astype(F32)
        lane = lax.broadcasted_iota(jnp.int32, (1, width), 1)
        empty = jnp.zeros((1, state), F32)
        for s in range(0, rows, 2):
            reads = []
            for t in range(2):
                for g in range(groups):
                    read = read_buf[s + t : s + t + 1, g * state : (g + 1) * state]
                    reads.append(jnp.concatenate([empty, read] if t else [read, empty], 1))
            reads.append(jnp.zeros((8 - 2 * groups, 2 * state), F32))
            found = lax.dot_general(
                jnp.concatenate(reads, 0).astype(BF16),
                state_ref[s // 2],
                (((1,), (1,)), ((), ())),
                preferred_element_type=F32,
            )
            for t in range(2):
                row = found[t * groups : t * groups + 1]
                for g in range(1, groups):
                    row = jnp.where(lane >= g * state, found[t * groups + g : t * groups + g + 1], row)
                sum_buf[s + t : s + t + 1, :] = row
        old_part = sum_buf[...]
        decay_ch = jnp.concatenate(
            [decay_ref[:, h * state : h * state + head_dim] for h in range(heads)], 1
        )
        both = []
        for g in range(groups):
            cols = slice(g * state, (g + 1) * state)
            inner = jnp.sum(b_act[:, cols] * c_act[:, cols], axis=-1, keepdims=True)
            both.append(fed[:, cols] * inner)
        ssm_out = decay_ch * old_part + jnp.concatenate(both, 1) + skip_ref[0:1] * x_act
        gated = ssm_out * silu(fresh[:, :width])
        gain = gain_ref[...]
        mixed = []
        for g in range(groups):
            cols = slice(g * state, (g + 1) * state)
            mixed.append(gated[:, cols] * row_scale(gated[:, cols]) * gain[:, cols])
        mixed = jnp.concatenate(mixed, 1).astype(BF16)
        mixed_out[...] = mixed
        for i, start in enumerate(half_rows(width, 1 - rank % CORES, model // width // CORES)):
            part = jnp.dot(mixed, out_ref[:, pl.ds(start, width)], preferred_element_type=F32)
            other_out[:, i * width : (i + 1) * width] = part.astype(BF16)

    outs = [
        jax.ShapeDtypeStruct((rows, partials[0].shape[1]), BF16),
        jax.ShapeDtypeStruct((rows, width), F32),
        jax.ShapeDtypeStruct((rows, width), F32),
        jax.ShapeDtypeStruct((rows, width), BF16),
        jax.ShapeDtypeStruct((rows, model // CORES), BF16),
    ]
    operands = (
        *partials, scale, step, decay, skip, conv_old, conv_last, ssm_state, group_gain, out_proj,
    )
    scratch = [pltpu.VMEM((rows, width), F32), pltpu.VMEM((rows, width), F32)]
    return local_kernel(body, outs, operands, 2 * rows * width * model, scratch)


def mix_kept(mixed, out_proj):
    rows, width = mixed.shape
    model = out_proj.shape[1]

    def body(mixed_ref, out_ref, out):
        core = lax.axis_index("tp") % CORES
        for i, start in enumerate(half_rows(width, core, model // width // CORES)):
            out[:, i * width : (i + 1) * width] = jnp.dot(
                mixed_ref[...], out_ref[:, pl.ds(start, width)], preferred_element_type=F32
            )

    outs = [jax.ShapeDtypeStruct((rows, model // CORES), F32)]
    return local_kernel(body, outs, (mixed, out_proj), rows * width * model)[0]


def advance_state(ssm_state, decay, fed, written, projected, conv_state):
    rows, heads, head_dim, state = ssm_state.shape
    width = heads * head_dim
    groups = width // state
    per_group = heads // groups
    taps, kinds = conv_state.shape[:2]
    chunk = 8

    def body(state_ref, decay_ref, fed_ref, write_ref, proj_ref, conv_ref, out_hbm, conv_out, *scratch):
        buf, fresh, sems = scratch
        shift = pltpu.make_async_copy(
            conv_ref.at[1:], conv_out.at[: taps - 1], sems.at[rows // chunk]
        )
        shift.start()
        for j in range(kinds):
            fresh[j] = proj_ref[:, (j + 1) * width : (j + 2) * width]
        newest = pltpu.make_async_copy(fresh, conv_out.at[taps - 1], sems.at[rows // chunk + 1])
        newest.start()
        fed_cols = fed_ref[...].T
        copies = [shift, newest]
        for s in range(rows):
            for h in range(heads):
                g = h // per_group
                fade = decay_ref[s : s + 1, h * state : (h + 1) * state]
                write = write_ref[s : s + 1, g * state : (g + 1) * state]
                column = fed_cols[h * head_dim : (h + 1) * head_dim, s : s + 1]
                buf[s, h] = fade * state_ref[s, h] + column * write
            if s % chunk == chunk - 1:
                span = pl.ds(s - chunk + 1, chunk)
                done = pltpu.make_async_copy(buf.at[span], out_hbm.at[span], sems.at[s // chunk])
                done.start()
                copies.append(done)
        for copy in copies:
            copy.wait()

    outs = [
        jax.ShapeDtypeStruct(ssm_state.shape, F32),
        jax.ShapeDtypeStruct(conv_state.shape, conv_state.dtype),
    ]
    scratch = [
        pltpu.VMEM(ssm_state.shape, F32),
        pltpu.VMEM((kinds, rows, width), conv_state.dtype),
        pltpu.SemaphoreType.DMA((rows // chunk + 2,)),
    ]
    operands = (ssm_state, decay, fed, written, projected, conv_state)
    return local_kernel(body, outs, operands, 8 << 20, scratch, (), (0, 1))


def column_blocks(width, z_count, kept):
    rank = lax.axis_index("tp")
    z, core = rank // CORES, rank % CORES
    starts = []
    for step in range(z_count):
        same = (step == 0) == kept
        parity = core if same else 1 - core
        starts.append(pl.multiple_of((partner(z_count, z, step) * CORES + parity) * width, LANES))
    return starts


def dense_branch(mine, other, ffn_gain, gate, up, down, blend):
    rows = mine.shape[0]
    model = gate.shape[0]
    half = model // CORES
    tp_count = lax.axis_size("tp")
    width = model // tp_count
    z_count = tp_count // CORES

    def body(
        mine_ref, other_ref, gain_ref, gate_ref, up_ref, down_ref, blend_ref, mine_out, other_out, joined
    ):
        interleave(joined, [mine_ref], [other_ref], lax.axis_index("tp") % CORES, width)
        values = joined[...].astype(F32)
        normed = (values * row_scale(values) * gain_ref[...]).astype(BF16)
        gated = jnp.dot(normed, gate_ref[...], preferred_element_type=F32)
        raised = jnp.dot(normed, up_ref[...], preferred_element_type=F32)
        hidden = (silu(gated) * raised).astype(BF16)
        weight = jax.nn.sigmoid(
            jnp.sum(normed.astype(F32) * blend_ref[...].astype(F32), axis=-1, keepdims=True)
        )
        for kept, out in ((True, mine_out), (False, other_out)):
            for i, start in enumerate(column_blocks(width, z_count, kept)):
                part = jnp.dot(hidden, down_ref[:, pl.ds(start, width)], preferred_element_type=F32)
                out[:, i * width : (i + 1) * width] = part * weight

    outs = [jax.ShapeDtypeStruct((rows, half), F32)] * 2
    operands = (mine, other, ffn_gain, gate, up, down, blend)
    flops = 6 * rows * model * gate.shape[1]
    scratch = [pltpu.VMEM((rows, model), BF16)]
    return local_kernel(body, outs, operands, flops, scratch)


def down_blocks(hidden, down_ref, width, z_count, kept):
    ffe = down_ref.shape[1]
    for i, start in enumerate(column_blocks(width, z_count, kept)):
        result = None
        for j in range(down_ref.shape[0]):
            part = jnp.dot(
                hidden[:, j * ffe : (j + 1) * ffe],
                down_ref[j, :, pl.ds(start, width)],
                preferred_element_type=F32,
            )
            result = part if result is None else result + part
        yield slice(i * width, (i + 1) * width), result


def half_product(refs, gain_ref, mats, starts, width):
    half = width * len(starts)
    values = jnp.concatenate([r[:, :half] for r in refs], 0).astype(F32)
    gain = jnp.concatenate([gain_ref[:, pl.ds(s, width)] for s in starts], 1)
    scaled = (values * gain).astype(BF16)
    products = []
    for ref, j in mats:
        weights = jnp.concatenate([ref[j, pl.ds(s, width), :] for s in starts], 0)
        products.append(jnp.dot(scaled, weights, preferred_element_type=F32))
    return products, jnp.sum(values * values, axis=-1, keepdims=True)


def expert_first(first, ffn_gain, gate, up, down):
    count = len(first)
    every = first[0].shape[0] * count
    experts, model, ffe = gate.shape
    tp_count = lax.axis_size("tp")
    width = model // tp_count

    def body(*refs):
        gain_ref, gate_ref, up_ref, _, partial_out, square_out = refs[count:]
        starts = half_rows(width, lax.axis_index("tp") % CORES, tp_count // CORES)
        mats = [(ref, j) for j in range(experts) for ref in (gate_ref, up_ref)]
        products, squares = half_product(refs[:count], gain_ref, mats, starts, width)
        for i, product in enumerate(products):
            partial_out[:, i * ffe : (i + 1) * ffe] = product
        square_out[...] = jnp.broadcast_to(squares, square_out.shape)

    outs = [
        jax.ShapeDtypeStruct((every, 2 * experts * ffe), F32),
        jax.ShapeDtypeStruct((every, LANES), F32),
    ]
    flops = 2 * every * model * ffe * experts
    return local_kernel(body, outs, (*first, ffn_gain, gate, up, down), flops)


def expert_sent(partial, squares, tables, second, ffn_gain, gate, up, down, dense_mine):
    count = len(second)
    rows = second[0].shape[0]
    experts, model, ffe = gate.shape
    half = model // CORES
    tp_count = lax.axis_size("tp")
    width = model // tp_count
    z_count = tp_count // CORES
    total = experts * lax.axis_size("ep")

    def body(partial_ref, square_ref, *refs):
        table_refs, other_refs, refs = refs[:count], refs[count : 2 * count], refs[2 * count :]
        gain_ref, gate_ref, up_ref, down_ref, dense_ref, hidden_out, own_out, other_out = refs
        starts = half_rows(width, 1 - lax.axis_index("tp") % CORES, z_count)
        mats = [(ref, j) for j in range(experts) for ref in (gate_ref, up_ref)]
        products, others = half_product(other_refs, gain_ref, mats, starts, width)
        scale = lax.rsqrt((square_ref[:, :1] + others) / model + epsilon)
        products = [
            (p + partial_ref[:, i * ffe : (i + 1) * ffe]) * scale for i, p in enumerate(products)
        ]
        start = lax.axis_index("ep") * experts
        table = jnp.concatenate([r[:, half:].astype(F32) for r in table_refs], 0)
        lane = lax.broadcasted_iota(jnp.int32, table.shape, 1)
        for j in range(experts):
            gated, raised = products[2 * j], products[2 * j + 1]
            picked = (lane == start + j) | (lane == start + j + total)
            share = jnp.sum(jnp.where(picked, table, 0.0), axis=-1, keepdims=True)
            hidden_out[:, j * ffe : (j + 1) * ffe] = (silu(gated) * raised * share).astype(BF16)
        for cols, part in down_blocks(hidden_out, down_ref, width, z_count, True):
            own_out[:, cols] = part[:rows] + dense_ref[:, cols]
            other_out[:, cols] = part[rows:].astype(BF16)

    every = rows * count
    outs = [
        jax.ShapeDtypeStruct((every, experts * ffe), BF16),
        jax.ShapeDtypeStruct((rows, half), F32),
        jax.ShapeDtypeStruct((every - rows, half), BF16),
    ]
    operands = (partial, squares, *tables, *second, ffn_gain, gate, up, down, dense_mine)
    return local_kernel(body, outs, operands, 3 * every * model * ffe * experts)


def expert_kept(hidden, down, dense_other):
    every = hidden.shape[0]
    rows, half = dense_other.shape
    tp_count = lax.axis_size("tp")
    width = half * CORES // tp_count
    z_count = tp_count // CORES

    def body(hidden_ref, down_ref, dense_ref, own_out, out):
        for cols, part in down_blocks(hidden_ref, down_ref, width, z_count, False):
            own_out[:, cols] = (part[:rows] + dense_ref[:, cols]).astype(BF16)
            out[:, cols] = part[rows:]

    outs = [
        jax.ShapeDtypeStruct((rows, half), BF16),
        jax.ShapeDtypeStruct((every - rows, half), F32),
    ]
    flops = 2 * every * half * hidden.shape[1]
    return local_kernel(body, outs, (hidden, down, dense_other), flops)


def layer(
    residual,
    mixer_gain,
    gate_proj,
    input_proj,
    write_proj,
    read_proj,
    step_proj,
    conv_weight,
    step_bias,
    log_rate,
    skip_gain,
    group_gain,
    ssm_state,
    conv_state,
    out_proj,
    ffn_gain,
    routes,
    route_weight,
    expert_gate,
    expert_up,
    expert_down,
    dense_gate,
    dense_up,
    dense_down,
    blend_weight,
):
    rows = residual.shape[0]
    depth, width = gate_proj.shape
    heads = ssm_state.shape[1]
    ep_count, tp_count = lax.axis_size("ep"), lax.axis_size("tp")
    z_count = tp_count // CORES
    tp_rank = lax.axis_index("tp")
    z_rank = tp_rank // CORES
    ep_rank = lax.axis_index("ep")
    ep_steps, z_steps = range(1, ep_count), range(1, z_count)
    sizes = ep_count, tp_count
    expert_total = expert_gate.shape[0] * ep_count
    as_row = lambda vector: vector.reshape(1, -1)

    slices = [
        lax.dynamic_slice_in_dim(residual, partner(ep_count, ep_rank, k) * depth, depth, 1)
        for k in ep_steps
    ]
    blocks = [send_ep(s, *sizes, k, cross=True) for k, s in zip(ep_steps, slices)]
    conv_rows = conv_state.transpose(1, 2, 0, 3)
    (
        scale, step, decay, skip, resid_half, conv_old, conv_last, gain, own, depth_gain, table, conv_held,
        *weights,
    ) = head_terms(
        residual, as_row(mixer_gain), step_proj.T, as_row(step_bias), as_row(log_rate),
        as_row(skip_gain), conv_rows, routes.T, route_weight.T, conv_weight.transpose(1, 0, 2),
        as_row(group_gain), (gate_proj, input_proj, write_proj, read_proj), heads, width, expert_total,
    )
    partials = project((own, *blocks), depth_gain, weights)
    parts = [partials[0]] + [send_ep(partials[k], *sizes, k, back=True) for k in ep_steps]
    state, low_state, out_weight = load_state(ssm_state, out_proj)
    projected, fed, written, mixed, other = mix(
        parts, scale, step, decay, skip, conv_old, conv_last, low_state, gain, out_weight
    )

    summed = send_core(other, tp_count)
    mine = mix_kept(mixed, out_weight) + summed.astype(F32)
    shared = mine.astype(BF16)
    gathered = [send_z(shared, *sizes, k) for k in z_steps]
    new_state, new_conv = advance_state(state, decay, fed, written, projected, conv_held)
    new_conv = new_conv.transpose(2, 0, 1, 3)
    for part in gathered:
        mine = mine + part.astype(F32)
    resid_mid = (resid_half.astype(F32) + mine).astype(BF16)
    packed = jnp.concatenate((resid_mid, table), 1)

    seconds = [send_ep(packed, *sizes, k) for k in ep_steps]
    own_other = send_core(packed, tp_count)
    dense_mine, dense_other = dense_branch(
        packed, own_other, as_row(ffn_gain), dense_gate, dense_up, dense_down, as_row(blend_weight)
    )
    firsts = []
    for k, second in zip(ep_steps, seconds):
        cut = second[:, : resid_mid.shape[1]]
        firsts.append(send_core(cut, tp_count))
    tokens = (packed, *seconds)
    partial, squares = expert_first(tokens, as_row(ffn_gain), expert_gate, expert_up, expert_down)
    hidden, total, other = expert_sent(
        partial, squares, tokens, (own_other, *firsts), as_row(ffn_gain), expert_gate, expert_up,
        expert_down, dense_mine,
    )
    summed = send_core(other, tp_count)
    own_sent, kept = expert_kept(hidden, expert_down, dense_other)
    low = (kept + summed.astype(F32)).astype(BF16)
    total = total + send_core(own_sent, tp_count).astype(F32)
    for k in ep_steps:
        piece = low[(k - 1) * rows : k * rows]
        total = total + send_ep(piece, *sizes, k, cross=True, back=True).astype(F32)
    low = total.astype(BF16)
    result = lax.dynamic_slice_in_dim(resid_mid, z_rank * width, width, 1).astype(F32)
    result = result + total[:, :width]
    for k in z_steps:
        piece = low[:, k * width : (k + 1) * width]
        result = result + send_z(piece, *sizes, k, cross=True).astype(F32)
    return result.astype(BF16), new_state, new_conv


def solution(mesh):
    return jax.shard_map(
        layer,
        mesh=mesh,
        in_specs=(
            P("ep", None),
            P(),
            P("ep", "tp"),
            P("ep", "tp"),
            P("ep", "tp"),
            P("ep", "tp"),
            P(),
            P(),
            P(),
            P(),
            P(),
            P(),
            P("ep", "tp", None, None),
            P("ep", None, None, "tp"),
            P("tp", None),
            P(),
            P("ep", None),
            P("ep", None),
            P("ep", None, "tp"),
            P("ep", None, "tp"),
            P("ep", "tp", None),
            P(None, "tp"),
            P(None, "tp"),
            P("tp", None),
            P(),
        ),
        out_specs=(P("ep", "tp"), P("ep", "tp", None, None), P("ep", None, None, "tp")),
        check_vma=False,
    )
```
